32 devices in a mesh: kv: 8 (over z, y), tp: 4 (over x, core).
Axes of the slice: x: 2, y: 2, z: 4, core: 2. Of those that a mesh axis runs over, the one named last changes fastest.
Arguments:
- tokens: bfloat16 [64, 6, 4096], P('kv'), may hold values from -6 to 6
- norm_gain: float32 [4096], replicated, may hold values from 0.1 to 1.9
- w_query: bfloat16 [4096, 2048], P('kv', 'tp'), may hold values from -0.09375 to 0.09375
- w_key: bfloat16 [4096, 2048], P('kv', 'tp'), may hold values from -0.09375 to 0.09375
- w_value: bfloat16 [4096, 2048], P('kv', 'tp'), may hold values from -0.09375 to 0.09375
- w_outgate: bfloat16 [4096, 2048], P('kv', 'tp'), may hold values from -0.09375 to 0.09375
- w_gates: bfloat16 [4096, 2, 16], P('kv', None, 'tp'), may hold values from -0.09375 to 0.09375
- forget_bias: float32 [16], P('tp'), may hold values from 1 to 6
- head_gain: float32 [2048], P('tp'), may hold values from 0.1 to 1.9
- w_mix: bfloat16 [2048, 4096], P('tp', 'kv'), may hold values from -0.125 to 0.125
- state_cell: float32 [64, 16, 128, 128], P('kv', 'tp'), may hold values from -4 to 4
- state_norm: float32 [64, 16, 128], P('kv', 'tp'), may hold values from -4 to 4
- state_max: float32 [64, 16], P('kv', 'tp'), may hold values from -4 to 120
- pend_keys: bfloat16 [64, 6, 2048], P('kv', None, 'tp'), may hold values from -6 to 6
- pend_values: bfloat16 [64, 6, 2048], P('kv', None, 'tp'), may hold values from -6 to 6
- pend_gates: float32 [64, 6, 2, 16], P('kv', None, None, 'tp'), may hold values from -6 to 6
- accepted: int32 [64], P('kv'), may hold values from 0 to 6
Outputs:
- mixed: bfloat16 [64, 6, 4096], P('kv', None, 'tp')
- new_cell: float32 [64, 16, 128, 128], P('kv', 'tp')
- new_norm: float32 [64, 16, 128], P('kv', 'tp')
- new_max: float32 [64, 16], P('kv', 'tp')
The draws below stay inside these ranges and needn't reach their ends.
All inputs are finite; a program needn't handle non-finite values.
Results may differ from the reference program's by a relative error of at most 0.018.
Values may be sent and summed in bfloat16 or wider, within the bound.
A program may use at most 128 MiB of HBM per device.

```python
import jax
import jax.numpy as jnp
from jax import lax

D = 4096
HEADS = 16
HD = 128
PROPS = 6
BR_W = 2048
SEQS = 64
N_TP = 4


def draw_state_max(key, part):
    return jnp.clip(1.5 * jax.random.normal(key, (SEQS, HEADS), jnp.float32), -4.0, 4.0)


def with_ends(values, rng, smallest, top_value):
    longest = values.shape.index(max(values.shape))
    spots = []
    for shift in (0, 1):
        where = [jax.random.randint(jax.random.fold_in(rng, axis), (), 0, length) for axis, length in enumerate(values.shape)]
        where[longest] = (where[longest] + shift) % values.shape[longest]
        spots.append(tuple(where))
    return values.at[spots[0]].set(smallest).at[spots[1]].set(top_value)


def levels(rng, extent, split, least, largest):
    level = 1.0
    for dim, parts in split:
        heights = jax.random.uniform(jax.random.fold_in(jax.random.fold_in(rng, 6), dim), (parts,), jnp.float32, least / len(split), largest / len(split))
        level = level * jnp.repeat(jnp.exp(heights), extent[dim] // parts).reshape((-1,) + (1,) * (len(extent) - 1 - dim))
    return level


def bell_draw(stream_key, dims, spread, most, split=(), dtype=jnp.bfloat16):
    values = jax.random.normal(stream_key, dims, jnp.float32) * spread
    if len(split) > 0:
        values = levels(stream_key, dims, split, -0.22, 0.18) * values
    return jnp.clip(values, min=-most, max=most).astype(dtype)


def setup_inputs(seed: int = 0) -> dict:
    key_list = jax.random.split(jax.random.key(seed), 18)
    return {
        "tokens": bell_draw(key_list[0], (SEQS, PROPS, D), 1.0, 6.0, ((0, 8),)),
        "norm_gain": jnp.clip(1.0 + 0.18 * jax.random.normal(key_list[1], (D,), jnp.float32), 0.1, 1.9),
        "w_query": bell_draw(key_list[2], (D, BR_W), D ** -0.5, 0.09375, ((0, 8), (1, 4))),
        "w_key": bell_draw(key_list[3], (D, BR_W), D ** -0.5, 0.09375, ((0, 8), (1, 4))),
        "w_value": bell_draw(key_list[4], (D, BR_W), D ** -0.5, 0.09375, ((0, 8), (1, 4))),
        "w_outgate": bell_draw(key_list[5], (D, BR_W), D ** -0.5, 0.09375, ((0, 8), (1, 4))),
        "w_gates": bell_draw(key_list[6], (D, 2, HEADS), D ** -0.5, 0.09375, ((0, 8), (2, 4))),
        "forget_bias": jnp.clip(1.0 + 5.0 * jax.random.uniform(key_list[7], (HEADS,), jnp.float32) ** levels(key_list[7], (HEADS,), ((0, 4),), -0.2, 0.2), 1.0, 6.0),
        "head_gain": jnp.clip(1.0 + 0.18 * jax.random.normal(key_list[8], (BR_W,), jnp.float32), 0.1, 1.9),
        "w_mix": bell_draw(key_list[9], (BR_W, D), BR_W ** -0.5, 0.125, ((0, 4), (1, 8))),
        "state_cell": bell_draw(key_list[10], (SEQS, HEADS, HD, HD), 0.3, 4.0, ((0, 8), (1, 4)), jnp.float32),
        "state_norm": bell_draw(key_list[11], (SEQS, HEADS, HD), 0.3, 4.0, ((0, 8), (1, 4)), jnp.float32),
        "state_max": draw_state_max(jax.random.fold_in(key_list[17], 71), 0),
        "pend_keys": bell_draw(key_list[13], (SEQS, PROPS, BR_W), 1.0, 6.0, ((0, 8), (2, 4))),
        "pend_values": bell_draw(key_list[14], (SEQS, PROPS, BR_W), 1.0, 6.0, ((0, 8), (2, 4))),
        "pend_gates": bell_draw(key_list[15], (SEQS, PROPS, 2, HEADS), 1.0, 6.0, ((0, 8), (3, 4)), jnp.float32),
        "accepted": with_ends(jax.random.randint(key_list[16], (SEQS,), 0, PROPS + 1), jax.random.fold_in(key_list[16], 1), 0, PROPS).astype(jnp.int32),
    }


epsilon = 1e-06
very_low = -1e+30
highest = lax.Precision.HIGHEST

def fold_pending(cell_state, normer, stabilizer, key_rows, value_rows, gate_rows, forget_shift, accepted):
    proposals = key_rows.shape[1]
    accepted_mask = jnp.arange(proposals)[None, :, None] < accepted[:, None, None]
    log_in = jnp.where(accepted_mask, gate_rows[:, :, 0, :], very_low)
    log_keep = jnp.where(accepted_mask, jax.nn.log_sigmoid(gate_rows[:, :, 1, :] + forget_shift), 0.0)
    running = jnp.cumsum(log_keep, axis=1)
    block_total = running[:, -1]
    log_w = block_total[:, None, :] - running + log_in
    new_max = jnp.maximum(block_total + stabilizer, lax.optimization_barrier(jnp.max(log_w, axis=1)))
    weights = jnp.exp(log_w - new_max[:, None, :])
    carried = jnp.exp(block_total + stabilizer - new_max)
    weighted_keys = weights[..., None] * key_rows
    cell_new = carried[..., None, None] * cell_state + jnp.einsum('sphd,sphe->shde', weighted_keys, value_rows, precision=highest)
    norm_new = carried[..., None] * normer + lax.optimization_barrier(jnp.sum(weighted_keys, axis=1))
    return (cell_new, norm_new, new_max)

def read_block(queries, key_rows, value_rows, log_in, log_keep, cell_state, normer, stabilizer):
    proposals = queries.shape[1]
    causal = jnp.arange(proposals)[:, None] >= jnp.arange(proposals)[None, :]
    running_h = jnp.moveaxis(jnp.cumsum(log_keep, axis=1), 1, 2)
    input_h = jnp.moveaxis(log_in, 1, 2)
    log_d = jnp.where(causal, running_h[..., :, None] - running_h[..., None, :] + input_h[..., None, :], very_low)
    log_p = running_h + stabilizer[..., None]
    top_log = jnp.maximum(log_p, lax.optimization_barrier(jnp.max(log_d, axis=-1)))
    decays = jnp.exp(log_d - top_log[..., None])
    prior_w = jnp.exp(log_p - top_log)
    scores = jnp.einsum('sthd,suhd->shtu', queries, key_rows, precision=highest) * decays
    numerator = jnp.einsum('shtu,suhe->shte', scores, value_rows, precision=highest)
    numerator = numerator + prior_w[..., None] * jnp.einsum('sthd,shde->shte', queries, cell_state, precision=highest)
    denominator = lax.optimization_barrier(jnp.sum(scores, axis=-1)) + prior_w * jnp.einsum('sthd,shd->sht', queries, normer, precision=highest)
    hidden_out = numerator / jnp.maximum(jnp.abs(denominator), jnp.exp(-top_log))[..., None]
    return jnp.moveaxis(hidden_out, 1, 2)

def reference(tokens, norm_gain, w_query, w_key, w_value, w_outgate, w_gates, forget_bias, head_gain, w_mix, state_cell, state_norm, state_max, pend_keys, pend_values, pend_gates, accepted):
    sequences, proposals, model_width = tokens.shape
    flat_rows = tokens.reshape(sequences * proposals, model_width).astype(jnp.float32)
    row_scale = lax.rsqrt(lax.optimization_barrier(jnp.mean(flat_rows * flat_rows, axis=-1, keepdims=True)) + epsilon)
    scaled_in = (flat_rows * norm_gain).astype(jnp.bfloat16)

    def project(weight):
        return jnp.dot(scaled_in, weight, preferred_element_type=jnp.float32) * row_scale
    queries = project(w_query).astype(jnp.bfloat16)
    new_keys = project(w_key).astype(jnp.bfloat16)
    new_values = project(w_value).astype(jnp.bfloat16)
    outgate = project(w_outgate).astype(jnp.bfloat16)
    gate_pre = project(w_gates.reshape(model_width, 2 * HEADS)).reshape(sequences, proposals, 2, HEADS)

    def split_heads(array):
        return array.astype(jnp.float32).reshape(sequences, proposals, HEADS, HD)
    key_scale = HD ** (-0.5)
    cell_new, norm_new, new_max = fold_pending(state_cell, state_norm, state_max, split_heads(pend_keys) * key_scale, split_heads(pend_values), pend_gates, forget_bias, accepted)
    log_in = gate_pre[:, :, 0, :]
    log_keep = jax.nn.log_sigmoid(gate_pre[:, :, 1, :] + forget_bias)
    hidden = read_block(split_heads(queries), split_heads(new_keys) * key_scale, split_heads(new_values), log_in, log_keep, cell_new, norm_new, new_max)
    normed = hidden * lax.rsqrt(lax.optimization_barrier(jnp.mean(hidden * hidden, axis=-1, keepdims=True)) + epsilon) * head_gain.reshape(HEADS, HD)
    gated_rows = (jax.nn.sigmoid(split_heads(outgate)) * normed).astype(jnp.bfloat16)
    gated_rows = gated_rows.reshape(sequences * proposals, N_TP, BR_W // N_TP)
    group_parts = jnp.einsum('tgc,gcd->gtd', gated_rows.astype(jnp.float32), w_mix.reshape(N_TP, BR_W // N_TP, model_width).astype(jnp.float32)).astype(jnp.bfloat16)
    mixed_out = lax.optimization_barrier(jnp.sum(group_parts.astype(jnp.float32), axis=0)).astype(jnp.bfloat16)
    return (mixed_out.reshape(sequences, proposals, model_width), cell_new, norm_new, new_max)
```

```python
import functools

import jax
import jax.numpy as jnp
from jax import lax
from jax.experimental import pallas as pl
from jax.experimental.pallas import tpu as pltpu
from jax.sharding import PartitionSpec as P

epsilon = 1e-06
very_low = -1e30
highest = lax.Precision.HIGHEST


def shortened(shard):

    def short(part):
        return part.astype(jnp.bfloat16) if part.dtype == jnp.float32 else part

    return jax.tree.map(short, shard)


def from_partner(shard, axis, stride):
    return lax.ppermute(shard, axis, [(i, i ^ 1 << stride) for i in range(lax.axis_size(axis))])


def running_sum(values):
    steps = values.shape[1]
    upto = jnp.arange(steps)[:, None] >= jnp.arange(steps)[None, :]
    return jnp.sum(jnp.where(upto[None, :, :, None], values[:, None], 0.0), axis=2)


def fold_pending(
    cell_state, normer, stabilizer, key_rows, value_rows, gate_rows, forget_shift, accepted
):
    proposals = key_rows.shape[1]
    accepted_mask = jnp.arange(proposals)[None, :, None] < accepted[:, None, None]
    log_in = jnp.where(accepted_mask, gate_rows[:, :, 0, :], very_low)
    log_keep = jnp.where(
        accepted_mask, jax.nn.log_sigmoid(gate_rows[:, :, 1, :] + forget_shift), 0.0
    )
    running = running_sum(log_keep)
    block_total = running[:, -1]
    log_w = block_total[:, None, :] - running + log_in
    new_max = jnp.maximum(block_total + stabilizer, jnp.max(log_w, axis=1))
    weights = jnp.exp(log_w - new_max[:, None, :])
    carried = jnp.exp(block_total + stabilizer - new_max)
    weighted_keys = weights[..., None] * key_rows
    cell_new = carried[..., None, None] * cell_state + jnp.einsum(
        "sphd,sphe->shde", weighted_keys, value_rows, precision=highest
    )
    norm_new = carried[..., None] * normer + jnp.sum(weighted_keys, axis=1)
    return (cell_new, norm_new, new_max)


def read_block(queries, key_rows, value_rows, log_in, log_keep, cell_state, normer, stabilizer):
    proposals = queries.shape[1]
    causal = jnp.arange(proposals)[:, None] >= jnp.arange(proposals)[None, :]
    running_h = jnp.moveaxis(running_sum(log_keep), 1, 2)
    input_h = jnp.moveaxis(log_in, 1, 2)
    log_d = jnp.where(
        causal, running_h[..., :, None] - running_h[..., None, :] + input_h[..., None, :], very_low
    )
    log_p = running_h + stabilizer[..., None]
    top_log = jnp.maximum(log_p, jnp.max(log_d, axis=-1))
    decays = jnp.exp(log_d - top_log[..., None])
    prior_w = jnp.exp(log_p - top_log)
    scores = jnp.einsum("sthd,suhd->shtu", queries, key_rows, precision=highest) * decays
    numerator = jnp.einsum("shtu,suhe->shte", scores, value_rows, precision=highest)
    numerator = numerator + prior_w[..., None] * jnp.einsum(
        "sthd,shde->shte", queries, cell_state, precision=highest
    )
    denominator = jnp.sum(scores, axis=-1) + prior_w * jnp.einsum(
        "sthd,shd->sht", queries, normer, precision=highest
    )
    hidden_out = numerator / jnp.maximum(jnp.abs(denominator), jnp.exp(-top_log))[..., None]
    return jnp.moveaxis(hidden_out, 1, 2)


def digit_of(own, bit):
    return own // 2**bit % 2


def collect_digits(pieces, dims, own, bits, sender):
    for bit in bits:
        others = sender(pieces, bit)
        first = digit_of(own, bit) == 0
        pieces = tuple(
            (
                jnp.where(
                    first,
                    jnp.concatenate((mine, theirs), axis=dim),
                    jnp.concatenate((theirs, mine), axis=dim),
                )
                for mine, theirs, dim in zip(pieces, others, dims)
            )
        )
    return pieces


def butterfly(blocks, own, near_bits, sender):
    for bit in range(near_bits):
        axis = near_bits - 1 - bit
        mine_digit = digit_of(own, bit)
        kept = lax.dynamic_index_in_dim(blocks, mine_digit, axis, keepdims=False)
        outgoing = lax.dynamic_index_in_dim(blocks, 1 - mine_digit, axis, keepdims=False)
        arrived = sender(outgoing, bit)
        blocks = jnp.where(
            mine_digit == 0,
            jnp.stack((kept, arrived), axis=axis),
            jnp.stack((arrived, kept), axis=axis),
        )
    return blocks


def halving(terms, own, near_bits, sender):
    for bit in range(near_bits - 1, -1, -1):
        mine_digit = digit_of(own, bit)
        kept = tuple(
            (lax.dynamic_index_in_dim(term, mine_digit, 0, keepdims=False) for term in terms)
        )
        outgoing = tuple(
            (lax.dynamic_index_in_dim(term, 1 - mine_digit, 0, keepdims=False) for term in terms)
        )
        arrived = sender(outgoing, bit)
        terms = tuple((left + right for left, right in zip(kept, arrived)))
    return terms


def log_sigmoid(values):
    return jnp.minimum(values, 0.0) - jnp.log1p(jnp.exp(-jnp.abs(values)))


def flipped(index, bits):
    place = 1
    while place <= bits:
        if bits // place % 2:
            index = index + place * (1 - 2 * (index // place % 2))
        place *= 2
    return index


def step_kernel(
    ways,
    groups,
    seqs,
    tok_hbm,
    gain_hbm,
    wq_hbm,
    wk_hbm,
    wv_hbm,
    wo_hbm,
    wg_hbm,
    bias_hbm,
    head_gain_hbm,
    mix_hbm,
    cell_hbm,
    norm_hbm,
    max_hbm,
    pend_k_hbm,
    pend_v_hbm,
    pend_g_hbm,
    accepted_hbm,
    out_hbm,
    cell_out_hbm,
    norm_out_hbm,
    max_out_hbm,
    tok,
    gain,
    weights,
    wg,
    bias,
    head_gain,
    mix_w,
    cell,
    norm,
    stab,
    pend_k,
    pend_v,
    pend_g,
    accepted,
    out,
    cell_new,
    norm_new,
    max_new,
    tok_in,
    scaled,
    wg_in,
    sums,
    part_out,
    part_in,
    fold_rows,
    cell_high,
    cell_low,
    norm_head,
    decay,
    scale_col,
    gated,
    gated_in,
    swap_out,
    swap_in,
    kept,
    answer_out,
    answer_in,
    load_sem,
    store_sem,
    tok_send,
    tok_recv,
    fwd_send,
    fwd_recv,
    wg_send,
    wg_recv,
    part_send,
    part_recv,
    gated_send,
    gated_recv,
    swap_send,
    swap_recv,
    answer_send,
    answer_recv,
):
    me = lax.axis_index("kv")
    group = lax.axis_index("tp")
    across, core = group // 2, lax.rem(group, 2)
    side = lax.rem(me, 2)
    count, model_width = tok.shape
    rows = model_width // ways
    half = rows // 2
    chunks, span = weights.shape[0], weights.shape[2] // 4
    heads, head_size = norm.shape[1], norm.shape[2]
    per_chunk = heads // chunks
    proposals = count // seqs
    bits = ways.bit_length() - 1
    f32, bf16 = jnp.float32, jnp.bfloat16
    orders = [tuple(range(bits))] * chunks

    loads = {}

    def load(name, source, target):
        copy = pltpu.make_async_copy(source, target, load_sem.at[len(loads)])
        copy.start()
        loads[name] = copy

    load("tok", tok_hbm, tok)
    load("gain", gain_hbm, gain)
    for chunk in range(chunks):
        for index, source in enumerate((wq_hbm, wk_hbm, wv_hbm, wo_hbm)):
            load(
                ("weight", chunk, index),
                source.at[:, chunk * span : (chunk + 1) * span],
                weights.at[chunk, :, index * span : (index + 1) * span],
            )
    load("wg", wg_hbm, wg)
    load("bias", bias_hbm, bias)
    load("max", max_hbm, stab)
    load("pend_g", pend_g_hbm, pend_g)
    load("accepted", accepted_hbm, accepted)
    load("pend_k", pend_k_hbm, pend_k)
    load("pend_v", pend_v_hbm, pend_v)
    load("norm", norm_hbm, norm)
    load("cell", cell_hbm, cell)
    load("head_gain", head_gain_hbm, head_gain)
    load("mix", mix_hbm, mix_w)

    target = me // 2
    at_home = jnp.logical_and(target == group, core == 0)
    barrier = pltpu.get_barrier_semaphore()

    def signal(where):
        pl.semaphore_signal(
            barrier, inc=1, device_id=where, device_id_type=pl.DeviceIdType.MESH
        )

    partner = {"tp": 2 * across + 1 - core}
    for shift in range(1, ways):
        signal({"kv": flipped(me, shift)})
    signal(partner)
    for which in range(2):
        sender = 2 * group + which
        sender_core = side + which - 2 * side * which
        for other in range(groups // 2):
            sender_group = 2 * other + sender_core

            @pl.when(jnp.logical_or(sender != me, sender_group != group))
            def _():
                signal({"kv": sender, "tp": sender_group})

    @pl.when(at_home)
    def _():
        pl.semaphore_wait(barrier, ways + ways // 2 - 1)

    @pl.when(jnp.logical_not(at_home))
    def _():
        pl.semaphore_wait(barrier, ways + ways // 2)

    sends = []

    def remote(source, target_ref, send_sem, recv_sem, where):
        copy = pltpu.make_async_remote_copy(
            src_ref=source,
            dst_ref=target_ref,
            send_sem=send_sem,
            recv_sem=recv_sem,
            device_id=where,
            device_id_type=pl.DeviceIdType.MESH,
        )
        copy.start()
        sends.append(copy)
        return copy

    def columns(owner):
        return pl.ds(pl.multiple_of(owner * rows, rows), rows)

    halves = pl.ds(pl.multiple_of(core * half, half), half)

    tok_copies, fwd_copies, wg_copies = {}, {}, {}
    loads["tok"].wait()
    whole_first = 1

    def send_tokens(shift):
        there = flipped(me, shift)
        if shift == whole_first:
            source, place = tok.at[:, columns(there)], tok_in.at[shift]
        else:
            source = tok.at[:, pl.ds(pl.multiple_of(there * rows + core * half, half), half)]
            place = tok_in.at[shift, :, halves]
        tok_copies[shift] = remote(
            source, place, tok_send.at[shift], tok_recv.at[shift], {"kv": there}
        )

    first_sends = [shift for shift in range(ways - 1, 1, -1) if shift % 2]
    keepers = [shift for shift in range(ways - 1, 0, -1) if not shift % 2]
    for shift in [whole_first] + first_sends + keepers:
        send_tokens(shift)
    loads["wg"].wait()
    for shift in range(1, ways):
        wg_copies[shift] = remote(
            wg, wg_in.at[shift], wg_send.at[shift], wg_recv.at[shift], {"kv": flipped(me, shift)}
        )

    loads["gain"].wait()
    own_gain = gain[:, columns(me)]

    def scale_block(shift, block):
        scaled[shift] = (block.astype(f32) * own_gain).astype(bf16)

    def forward(shift):
        tok_copies[shift].wait_recv()
        place = tok_in.at[shift, :, halves]
        fwd_copies[shift] = remote(
            place, place, fwd_send.at[shift], fwd_recv.at[shift], partner
        )

    def arrive(shift):
        if shift == whole_first:
            tok_copies[shift].wait_recv()
        else:
            fwd_copies[shift].wait_recv()
        scale_block(shift, tok_in[shift])

    def product(chunk, shift):
        return jnp.dot(scaled[shift], weights[chunk], preferred_element_type=f32)

    part_copies = {}

    def send_part(chunk, shift, bit, value):
        part_out[chunk, shift] = value.astype(bf16)
        part_copies[chunk, shift] = remote(
            part_out.at[chunk, shift],
            part_in.at[chunk, shift],
            part_send.at[chunk, shift],
            part_recv.at[chunk, shift],
            {"kv": flipped(me, 1 << bit)},
        )

    def first_send(chunk, shift):
        send_part(chunk, shift, orders[chunk][0], product(chunk, shift))

    scale_block(0, tok[:, columns(me)])
    squares = jnp.zeros((count, 1), f32)
    for step in range(ways):
        part = tok[:, step * rows : (step + 1) * rows].astype(f32)
        squares = squares + jnp.sum(part * part, axis=1, keepdims=True)
    row_scale = lax.rsqrt(squares / model_width + epsilon)
    scale_col[...] = jnp.broadcast_to(row_scale, scale_col.shape)

    for chunk in range(chunks):
        for index in range(4):
            loads["weight", chunk, index].wait()

    arrive(whole_first)
    for chunk in range(chunks):
        first_send(chunk, whole_first)
    for shift in first_sends:
        forward(shift)

    def eye(size):
        across_rows = lax.broadcasted_iota(jnp.int32, (size, size), 0)
        return across_rows == lax.broadcasted_iota(jnp.int32, (size, size), 1)

    def fold_gates():
        for name in ("bias", "max", "pend_g", "accepted"):
            loads[name].wait()
        bias_col = jnp.sum(
            jnp.where(eye(heads), jnp.broadcast_to(bias[...], (heads, heads)), 0.0),
            axis=1,
            keepdims=True,
        )
        log_in, running = [], []
        total = jnp.zeros((heads, seqs), f32)
        for step in range(proposals):
            taken = jnp.broadcast_to(step < accepted[...], (heads, seqs))
            log_in.append(jnp.where(taken, pend_g[step, 0], very_low))
            total = total + jnp.where(taken, log_sigmoid(pend_g[step, 1] + bias_col), 0.0)
            running.append(total)
        log_w = [total - at + ins for at, ins in zip(running, log_in)]
        carried_log = total + stab[...]
        top = carried_log
        for values in log_w:
            top = jnp.maximum(top, values)
        max_new[...] = top
        fold_rows[...] = jnp.zeros(fold_rows.shape, f32)
        pieces = [jnp.exp(values - top) for values in log_w]
        pieces = pieces + [jnp.exp(carried_log - top), top]
        for index, piece in enumerate(pieces):
            fold_rows[index * heads : (index + 1) * heads, 0:seqs] = piece
        return fold_rows[...].T[:seqs]

    stores = []

    def store(source, target_ref):
        copy = pltpu.make_async_copy(source, target_ref, store_sem.at[len(stores)])
        copy.start()
        stores.append(copy)

    key_scale = head_size ** (-0.5)

    def fold_head(cols, head):
        lanes = slice(head * head_size, (head + 1) * head_size)
        keys = pend_k[:, lanes].astype(f32)
        weighted = []
        carried = jnp.broadcast_to(
            cols[:, proposals * heads + head : proposals * heads + head + 1], (seqs, head_size)
        )
        key_sum = carried * norm[:, head, :]
        for step in range(proposals):
            weight = cols[:, step * heads + head : step * heads + head + 1]
            rows_at = keys[step * seqs : (step + 1) * seqs] * key_scale * weight
            weighted.append(rows_at)
            key_sum = key_sum + rows_at
        norm_head[head] = key_sum
        norm_new[:, head, :] = key_sum
        padding = jnp.zeros((head_size - count, head_size), f32)
        turned = jnp.concatenate(weighted + [padding], axis=0).T
        value_rows = jnp.concatenate(
            [pend_v[:, lanes].astype(f32), padding], axis=0
        ).astype(bf16)
        value_rows = jnp.concatenate([value_rows, value_rows], axis=0)
        high = turned.astype(bf16).astype(f32)
        low = turned - high
        lane = lax.rem(lax.broadcasted_iota(jnp.int32, turned.shape, 1), seqs)
        for seq in range(seqs):
            mine = lane == seq
            left = jnp.concatenate(
                [jnp.where(mine, high, 0.0).astype(bf16), jnp.where(mine, low, 0.0).astype(bf16)],
                axis=1,
            )
            update = jnp.dot(left, value_rows, preferred_element_type=f32)
            result = carried[seq : seq + 1] * cell[seq, head] + update
            cell_new[seq, head] = result
            upper = result.astype(bf16)
            at = slice(seq * head_size, (seq + 1) * head_size)
            cell_high[head, at, :] = upper
            cell_low[head, at, :] = (result - upper.astype(f32)).astype(bf16)

    cols = fold_gates()
    for shift in first_sends:
        arrive(shift)
    for chunk in range(chunks):
        for shift in first_sends:
            first_send(chunk, shift)
    for shift in keepers:
        forward(shift)
    for name in ("pend_k", "pend_v", "norm", "cell"):
        loads[name].wait()
    for head in range(heads):
        fold_head(cols, head)
    store(cell_new, cell_out_hbm)
    store(norm_new, norm_out_hbm)
    store(max_new, max_out_hbm)

    for shift in keepers:
        arrive(shift)
    for chunk in range(chunks):
        for shift in keepers + [0]:
            sums[chunk, shift // 2] = product(chunk, shift)

    contract = (((1,), (1,)), ((), ()))
    gates = [jnp.zeros((count, heads), f32)] * 2
    for shift in range(ways):
        owner = flipped(me, shift)
        if shift:
            wg_copies[shift].wait_recv()
            block = (tok[:, columns(owner)].astype(f32) * gain[:, columns(owner)]).astype(bf16)
        else:
            block = scaled[0]
        for part in range(2):
            right = wg_in[shift, part] if shift else wg[part]
            gates[part] = gates[part] + lax.dot_general(
                block, right, contract, preferred_element_type=f32
            )

    def read_gates():
        stabilizer = cols[:, (proposals + 1) * heads : (proposals + 2) * heads]
        log_in, running = [], []
        total = jnp.zeros((seqs, heads), f32)
        scale = scale_col[:, :1]
        gate_in, gate_keep = gates[0] * scale, gates[1] * scale
        index = 0
        for step in range(proposals):
            at = slice(step * seqs, (step + 1) * seqs)
            log_in.append(gate_in[at])
            total = total + log_sigmoid(gate_keep[at] + bias[...])
            running.append(total)
            log_p = total + stabilizer
            log_d = [total - running[past] + log_in[past] for past in range(step + 1)]
            top = log_p
            for values in log_d:
                top = jnp.maximum(top, values)
            for values in log_d + [log_p, None]:
                decay[index, :, :heads] = jnp.exp(-top if values is None else values - top)
                index += 1

    read_gates()

    gated_copies = {}

    def send_gated(chunk, shift, there):
        place = slice(chunk * span, (chunk + 1) * span)
        source = gated.at[:, place]
        gated_copies[chunk, shift] = remote(
            source,
            gated_in.at[shift, :, place],
            gated_send.at[chunk, shift],
            gated_recv.at[chunk, shift],
            {"kv": there},
        )

    def forward_gated(chunk, shift):
        place = slice(chunk * span, (chunk + 1) * span)
        gated_copies[chunk, shift].wait_recv()
        gated_copies[chunk, shift + 1] = remote(
            gated_in.at[shift, :, place],
            gated_in.at[shift + 1, :, place],
            gated_send.at[chunk, shift + 1],
            gated_recv.at[chunk, shift + 1],
            {"kv": flipped(me, 1)},
        )

    def read_head(chunk, local, flat):
        head = chunk * per_chunk + local
        scale = scale_col[...]

        def piece(index):
            at = index * span + local * head_size
            return (flat[:, at : at + head_size] * scale).astype(bf16).astype(f32)

        query, key, value, outgate = (piece(index) for index in range(4))
        key = key * key_scale
        sequence = lax.rem(lax.broadcasted_iota(jnp.int32, query.shape, 0), seqs)
        spread = jnp.concatenate(
            [jnp.where(sequence == seq, query, 0.0).astype(bf16) for seq in range(seqs)], axis=1
        )
        prior = jnp.dot(spread, cell_high[head], preferred_element_type=f32)
        prior = prior + jnp.dot(spread, cell_low[head], preferred_element_type=f32)
        normer = norm_head[head]
        hidden = []
        index = 0
        for step in range(proposals):
            at = slice(step * seqs, (step + 1) * seqs)
            now = query[at]
            numerator, denominator = None, None

            def factor(which):
                return decay[which, :, head : head + 1]

            for past in range(step + 1):
                before = slice(past * seqs, (past + 1) * seqs)
                score = jnp.sum(now * key[before], axis=1, keepdims=True) * factor(index + past)
                term = score * value[before]
                numerator = term if numerator is None else numerator + term
                denominator = score if denominator is None else denominator + score
            prior_w = factor(index + step + 1)
            numerator = numerator + prior_w * prior[at]
            denominator = denominator + prior_w * jnp.sum(now * normer, axis=1, keepdims=True)
            floor = factor(index + step + 2)
            hidden.append(numerator / jnp.maximum(jnp.abs(denominator), floor))
            index += step + 3
        hidden = jnp.concatenate(hidden, axis=0)
        normed = hidden * lax.rsqrt(jnp.mean(hidden * hidden, axis=1, keepdims=True) + epsilon)
        lanes = slice(head * head_size, (head + 1) * head_size)
        normed = normed * head_gain[:, lanes]
        gated[:, lanes] = (jax.nn.sigmoid(outgate) * normed).astype(bf16)

    def take(chunk, stage):
        bit = 1 << orders[chunk][stage]
        done = sum(1 << orders[chunk][early] for early in range(stage + 1))
        later = [1 << b for b in orders[chunk][stage + 1 :]]
        places = [shift for shift in range(ways) if not shift & done]
        places.sort(key=lambda shift: tuple(-(shift // b % 2) for b in later))
        for shift in places:
            part_copies[chunk, shift + bit].wait_recv()
            value = sums[chunk, shift // 2] + part_in[chunk, shift + bit].astype(f32)
            if stage + 1 < bits and shift & later[0]:
                send_part(chunk, shift, orders[chunk][stage + 1], value)
            elif stage + 1 < bits:
                sums[chunk, shift // 2] = value
            else:
                for local in range(per_chunk):
                    read_head(chunk, local, value)

    loads["head_gain"].wait()
    loads["mix"].wait()
    last = chunks - 1
    for tick in range(chunks + bits):
        for stage in range(bits):
            chunk = tick - stage
            if 0 <= chunk < chunks:
                take(chunk, stage)
                if stage == bits - 1:
                    for shift in range(ways - 1, 0, -1):
                        if chunk == last or shift == 1 or not shift % 2:
                            send_gated(chunk, shift, flipped(me, shift))
        chunk = tick - bits
        if 0 <= chunk < last:
            for shift in range(ways - 2, 0, -2):
                forward_gated(chunk, shift)

    def mixed(block):
        return jnp.dot(block, mix_w[...], preferred_element_type=f32)

    swap_copies = {}
    first_core = core == 0
    pairs = list(range(ways // 2 - 1, -1, -1))
    for pair in pairs:
        values = []
        for shift in (2 * pair, 2 * pair + 1):
            if shift:
                for chunk in range(chunks):
                    gated_copies[chunk, shift].wait_recv() if (
                        chunk == last or shift % 2
                    ) else None
                values.append(mixed(gated_in[shift]))
            else:
                values.append(mixed(gated[...]))
        kept[pair] = jnp.where(first_core, values[0], values[1]).astype(bf16)
        swap_out[pair] = jnp.where(first_core, values[1], values[0]).astype(bf16)
        swap_copies[pair] = remote(
            swap_out.at[pair], swap_in.at[pair], swap_send.at[pair], swap_recv.at[pair], partner
        )

    spot = side * (groups // 2) + across

    def answer(pair):
        base = flipped(me, 2 * pair)
        owner = base + core * (1 - 2 * side)
        return pltpu.make_async_remote_copy(
            src_ref=answer_out.at[pair],
            dst_ref=answer_in.at[spot],
            send_sem=answer_send.at[pair],
            recv_sem=answer_recv.at[spot],
            device_id={"kv": owner, "tp": target},
            device_id_type=pl.DeviceIdType.MESH,
        )

    at_own = pltpu.make_async_copy(answer_out.at[0], answer_in.at[spot], answer_recv.at[spot])
    for pair in pairs:
        swap_copies[pair].wait_recv()
        answer_out[pair] = (kept[pair].astype(f32) + swap_in[pair].astype(f32)).astype(bf16)
        if pair:
            copy = answer(pair)
            copy.start()
            sends.append(copy)
        else:

            @pl.when(at_home)
            def _():
                at_own.start()

            @pl.when(jnp.logical_not(at_home))
            def _():
                answer(0).start()

    width = mix_w.shape[1]
    for which in range(2):
        total = None
        for other in range(groups // 2):
            slot = which * (groups // 2) + other
            pltpu.make_async_copy(
                answer_out.at[0], answer_in.at[slot], answer_recv.at[slot]
            ).wait()
            term = answer_in[slot].astype(f32)
            total = term if total is None else total + term
        out[:, which * width : (which + 1) * width] = total.astype(bf16)
    store(out, out_hbm)
    for copy in sends:
        copy.wait_send()

    @pl.when(jnp.logical_not(at_home))
    def _():
        answer(0).wait_send()

    for copy in stores:
        copy.wait()


def one_step(
    tokens,
    norm_gain,
    weights,
    w_gates,
    forget_bias,
    head_gain,
    w_mix,
    state_cell,
    state_norm,
    state_max,
    pend_keys,
    pend_values,
    pend_gates,
    accepted,
):
    ways, groups = lax.axis_size("kv"), lax.axis_size("tp")
    seqs, proposals, model_width = tokens.shape
    count = seqs * proposals
    rows, width = weights[0].shape
    heads, head_size = state_norm.shape[1:]
    chunks = heads
    span = width // chunks
    f32, bf16 = jnp.float32, jnp.bfloat16

    def by_proposal(array):
        return array.transpose(1, 0, 2).reshape(count, array.shape[2])

    operands = (
        by_proposal(tokens),
        norm_gain[None, :],
        *weights,
        w_gates.transpose(1, 2, 0),
        forget_bias[None, :],
        head_gain[None, :],
        w_mix,
        state_cell,
        state_norm,
        state_max.T,
        by_proposal(pend_keys),
        by_proposal(pend_values),
        pend_gates.transpose(1, 2, 3, 0),
        accepted[None, :],
    )
    out_shape = (
        jax.ShapeDtypeStruct((count, ways // groups * width), bf16),
        jax.ShapeDtypeStruct(state_cell.shape, f32),
        jax.ShapeDtypeStruct(state_norm.shape, f32),
        jax.ShapeDtypeStruct((heads, seqs), f32),
    )
    held = [jax.ShapeDtypeStruct(array.shape, array.dtype) for array in operands]
    held = held[:2] + [jax.ShapeDtypeStruct((chunks, rows, 4 * span), bf16)] + held[6:]
    held = held + list(out_shape)
    block = (ways, count, rows)
    scratch = [pltpu.VMEM(array.shape, array.dtype) for array in held]
    scratch += [
        pltpu.VMEM(block, bf16),
        pltpu.VMEM(block, bf16),
        pltpu.VMEM((ways, 2, heads, rows), bf16),
        pltpu.VMEM((chunks, ways // 2, count, 4 * span), f32),
        pltpu.VMEM((chunks, ways, count, 4 * span), bf16),
        pltpu.VMEM((chunks, ways, count, 4 * span), bf16),
        pltpu.VMEM(((proposals + 2) * heads, 128), f32),
        pltpu.VMEM((heads, seqs * head_size, head_size), bf16),
        pltpu.VMEM((heads, seqs * head_size, head_size), bf16),
        pltpu.VMEM((heads, seqs, head_size), f32),
        pltpu.VMEM((proposals * (proposals + 5) // 2, seqs, 128), f32),
        pltpu.VMEM((count, head_size), f32),
        pltpu.VMEM((count, width), bf16),
        pltpu.VMEM((ways, count, width), bf16),
    ]
    scratch += [pltpu.VMEM((ways // 2, count, width), bf16)] * 5
    dma = pltpu.SemaphoreType.DMA
    scratch += [dma((len(operands) + 4 * chunks,)), dma((8,))]
    scratch += [dma((ways,))] * 6
    scratch += [dma((chunks, ways))] * 4
    scratch += [dma((ways,))] * 4
    anywhere = pl.BlockSpec(memory_space=pl.ANY)
    mixed_out, cell_new, norm_new, max_new = pl.pallas_call(
        functools.partial(step_kernel, ways, groups, seqs),
        out_shape=out_shape,
        in_specs=[anywhere] * len(operands),
        out_specs=(anywhere,) * 4,
        scratch_shapes=scratch,
        compiler_params=pltpu.CompilerParams(collective_id=0, has_side_effects=True),
    )(*operands)
    mixed_out = mixed_out.reshape(proposals, seqs, -1).transpose(1, 0, 2)
    return mixed_out, cell_new, norm_new, max_new.T


def project_by_digits(flat_rows, norm_gain, weights, w_mix):
    token_count, model_width = flat_rows.shape
    shard_rows = weights[0].shape[0]
    own = lax.axis_index("kv")
    kv_bits = lax.axis_size("kv").bit_length() - 1
    near_bits = kv_bits // 2
    near = 2**near_bits
    far = lax.axis_size("kv") // near
    digit_shape = (2,) * near_bits
    collected = collect_digits(
        weights + (w_mix,),
        (0, 0, 0, 0, 0, 1),
        own,
        range(near_bits, kv_bits),
        lambda parts, bit: jax.tree.map(
            lambda part, own: part.astype(own.dtype),
            from_partner(shortened(parts), "kv", bit),
            parts,
        ),
    )
    far_mix = collected[5]
    token_digits = jnp.moveaxis(flat_rows.reshape(token_count, far, near, shard_rows), 2, 0)
    token_digits = token_digits.reshape(digit_shape + (token_count, far, shard_rows))
    arrived = butterfly(
        token_digits, own, near_bits, lambda part, bit: from_partner(part, "kv", bit)
    )
    gathered = arrived.reshape(near * token_count, far * shard_rows)
    gain_part = lax.dynamic_index_in_dim(
        norm_gain.reshape(far, near, shard_rows), own % near, 1, keepdims=False
    ).reshape(far * shard_rows)
    widened = gathered.astype(jnp.float32)
    scaled_in = (widened * gain_part).astype(jnp.bfloat16)
    partials = tuple(
        (
            jnp.dot(scaled_in, weight, preferred_element_type=jnp.float32).reshape(
                digit_shape + (token_count, weight.shape[1])
            )
            for weight in collected[:5]
        )
    )
    part_squares = jnp.sum(widened * widened, axis=-1).reshape(digit_shape + (token_count,))
    summed = halving(
        partials + (part_squares,),
        own,
        near_bits,
        lambda parts, bit: jax.tree.map(
            lambda part, own: part.astype(own.dtype),
            from_partner(shortened(parts), "kv", bit),
            parts,
        ),
    )
    totals = summed[:5]
    sum_squares = summed[5]
    row_scale = lax.rsqrt(sum_squares / model_width + epsilon)[:, None]
    return (
        tuple((total * row_scale).astype(jnp.bfloat16) for total in totals[:4]),
        totals[4] * row_scale,
        far_mix,
    )


def mix_by_digits(gated_rows, far_mix, model_width):
    token_count = gated_rows.shape[0]
    shard_rows = model_width // lax.axis_size("kv")
    own = lax.axis_index("kv")
    kv_bits = lax.axis_size("kv").bit_length() - 1
    near_bits = kv_bits // 2
    near = 2**near_bits
    far = lax.axis_size("kv") // near
    digit_shape = (2,) * near_bits
    near_gated = collect_digits(
        (gated_rows,),
        (0,),
        own,
        range(near_bits),
        lambda parts, bit: jax.tree.map(
            lambda part, own: part.astype(own.dtype),
            from_partner(shortened(parts), "kv", bit),
            parts,
        ),
    )[0]
    group_part = jnp.dot(near_gated, far_mix, preferred_element_type=jnp.float32).astype(
        jnp.bfloat16
    )
    group_part = group_part.reshape(digit_shape + (token_count, far, shard_rows))
    placed = butterfly(group_part, own, near_bits, lambda part, bit: from_partner(part, "kv", bit))
    placed = placed.reshape(near, token_count, far, shard_rows).transpose(1, 2, 0, 3)
    partial_out = placed.reshape(token_count, model_width).astype(jnp.float32)
    mixed_out = lax.psum_scatter(
        partial_out.astype(jnp.bfloat16), "tp", scatter_dimension=1, tiled=True
    )
    return mixed_out


def shards(
    tokens,
    norm_gain,
    w_query,
    w_key,
    w_value,
    w_outgate,
    w_gates,
    forget_bias,
    head_gain,
    w_mix,
    state_cell,
    state_norm,
    state_max,
    pend_keys,
    pend_values,
    pend_gates,
    accepted,
):
    sequences, proposals, model_width = tokens.shape
    token_count = sequences * proposals
    local_heads = forget_bias.shape[0]
    head_size = state_cell.shape[-1]
    shard_rows = w_query.shape[0]
    weights = (w_query, w_key, w_value, w_outgate)
    ways, groups = lax.axis_size("kv"), lax.axis_size("tp")
    direct = (
        shard_rows % 256 == 0
        and w_mix.shape[1] == shard_rows
        and w_query.shape[1] == shard_rows
        and ways == 2 * groups
        and groups % 2 == 0
        and sequences == 8
        and head_size == 128
        and token_count <= head_size
    )
    if direct:
        return one_step(
            tokens,
            norm_gain,
            weights,
            w_gates,
            forget_bias,
            head_gain,
            w_mix,
            state_cell,
            state_norm,
            state_max,
            pend_keys,
            pend_values,
            pend_gates,
            accepted,
        )
    flat_gates = w_gates.reshape(shard_rows, -1)
    flat_rows = tokens.reshape(token_count, model_width)
    projected, gate_pre, far_mix = project_by_digits(
        flat_rows, norm_gain, weights + (flat_gates,), w_mix
    )
    queries, new_keys, new_values, outgate = projected
    gate_pre = gate_pre.reshape(sequences, proposals, 2, local_heads)

    def split_heads(array):
        return array.astype(jnp.float32).reshape(sequences, proposals, local_heads, head_size)

    key_scale = head_size ** (-0.5)
    cell_new, norm_new, new_max = fold_pending(
        state_cell,
        state_norm,
        state_max,
        split_heads(pend_keys) * key_scale,
        split_heads(pend_values),
        pend_gates,
        forget_bias,
        accepted,
    )
    log_in = gate_pre[:, :, 0, :]
    log_keep = jax.nn.log_sigmoid(gate_pre[:, :, 1, :] + forget_bias)
    hidden = read_block(
        split_heads(queries),
        split_heads(new_keys) * key_scale,
        split_heads(new_values),
        log_in,
        log_keep,
        cell_new,
        norm_new,
        new_max,
    )
    normed = hidden * lax.rsqrt(jnp.mean(hidden * hidden, axis=-1, keepdims=True) + epsilon)
    normed = normed * head_gain.reshape(local_heads, head_size)
    gated_rows = (jax.nn.sigmoid(split_heads(outgate)) * normed).astype(jnp.bfloat16)
    gated_rows = gated_rows.reshape(token_count, local_heads * head_size)
    mixed_out = mix_by_digits(gated_rows, far_mix, model_width)
    return (mixed_out.reshape(sequences, proposals, -1), cell_new, norm_new, new_max)


def solution(mesh):
    return jax.shard_map(
        shards,
        mesh=mesh,
        in_specs=(
            P("kv", None, None),
            P(),
            P("kv", "tp"),
            P("kv", "tp"),
            P("kv", "tp"),
            P("kv", "tp"),
            P("kv", None, "tp"),
            P("tp"),
            P("tp"),
            P("tp", "kv"),
            P("kv", "tp", None, None),
            P("kv", "tp", None),
            P("kv", "tp"),
            P("kv", None, "tp"),
            P("kv", None, "tp"),
            P("kv", None, None, "tp"),
            P("kv"),
        ),
        out_specs=(
            P("kv", None, "tp"),
            P("kv", "tp", None, None),
            P("kv", "tp", None),
            P("kv", "tp"),
        ),
        check_vma=False,
    )
```

```python
import functools

import jax
import jax.numpy as jnp
from jax import lax
from jax.experimental import pallas as pl
from jax.experimental.pallas import tpu as pltpu
from jax.sharding import PartitionSpec as P

epsilon = 1e-06
very_low = -1e30
highest = lax.Precision.HIGHEST


def shortened(shard):

    def short(part):
        return part.astype(jnp.bfloat16) if part.dtype == jnp.float32 else part

    return jax.tree.map(short, shard)


def from_partner(shard, axis, stride):
    return lax.ppermute(shard, axis, [(i, i ^ 1 << stride) for i in range(lax.axis_size(axis))])


def running_sum(values):
    steps = values.shape[1]
    upto = jnp.arange(steps)[:, None] >= jnp.arange(steps)[None, :]
    return jnp.sum(jnp.where(upto[None, :, :, None], values[:, None], 0.0), axis=2)


def fold_pending(
    cell_state, normer, stabilizer, key_rows, value_rows, gate_rows, forget_shift, accepted
):
    proposals = key_rows.shape[1]
    accepted_mask = jnp.arange(proposals)[None, :, None] < accepted[:, None, None]
    log_in = jnp.where(accepted_mask, gate_rows[:, :, 0, :], very_low)
    log_keep = jnp.where(
        accepted_mask, jax.nn.log_sigmoid(gate_rows[:, :, 1, :] + forget_shift), 0.0
    )
    running = running_sum(log_keep)
    block_total = running[:, -1]
    log_w = block_total[:, None, :] - running + log_in
    new_max = jnp.maximum(block_total + stabilizer, jnp.max(log_w, axis=1))
    weights = jnp.exp(log_w - new_max[:, None, :])
    carried = jnp.exp(block_total + stabilizer - new_max)
    weighted_keys = weights[..., None] * key_rows
    cell_new = carried[..., None, None] * cell_state + jnp.einsum(
        "sphd,sphe->shde", weighted_keys, value_rows, precision=highest
    )
    norm_new = carried[..., None] * normer + jnp.sum(weighted_keys, axis=1)
    return (cell_new, norm_new, new_max)


def read_block(queries, key_rows, value_rows, log_in, log_keep, cell_state, normer, stabilizer):
    proposals = queries.shape[1]
    causal = jnp.arange(proposals)[:, None] >= jnp.arange(proposals)[None, :]
    running_h = jnp.moveaxis(running_sum(log_keep), 1, 2)
    input_h = jnp.moveaxis(log_in, 1, 2)
    log_d = jnp.where(
        causal, running_h[..., :, None] - running_h[..., None, :] + input_h[..., None, :], very_low
    )
    log_p = running_h + stabilizer[..., None]
    top_log = jnp.maximum(log_p, jnp.max(log_d, axis=-1))
    decays = jnp.exp(log_d - top_log[..., None])
    prior_w = jnp.exp(log_p - top_log)
    scores = jnp.einsum("sthd,suhd->shtu", queries, key_rows, precision=highest) * decays
    numerator = jnp.einsum("shtu,suhe->shte", scores, value_rows, precision=highest)
    numerator = numerator + prior_w[..., None] * jnp.einsum(
        "sthd,shde->shte", queries, cell_state, precision=highest
    )
    denominator = jnp.sum(scores, axis=-1) + prior_w * jnp.einsum(
        "sthd,shd->sht", queries, normer, precision=highest
    )
    hidden_out = numerator / jnp.maximum(jnp.abs(denominator), jnp.exp(-top_log))[..., None]
    return jnp.moveaxis(hidden_out, 1, 2)


def digit_of(own, bit):
    return own // 2**bit % 2


def collect_digits(pieces, dims, own, bits, sender):
    for bit in bits:
        others = sender(pieces, bit)
        first = digit_of(own, bit) == 0
        pieces = tuple(
            (
                jnp.where(
                    first,
                    jnp.concatenate((mine, theirs), axis=dim),
                    jnp.concatenate((theirs, mine), axis=dim),
                )
                for mine, theirs, dim in zip(pieces, others, dims)
            )
        )
    return pieces


def butterfly(blocks, own, near_bits, sender):
    for bit in range(near_bits):
        axis = near_bits - 1 - bit
        mine_digit = digit_of(own, bit)
        kept = lax.dynamic_index_in_dim(blocks, mine_digit, axis, keepdims=False)
        outgoing = lax.dynamic_index_in_dim(blocks, 1 - mine_digit, axis, keepdims=False)
        arrived = sender(outgoing, bit)
        blocks = jnp.where(
            mine_digit == 0,
            jnp.stack((kept, arrived), axis=axis),
            jnp.stack((arrived, kept), axis=axis),
        )
    return blocks


def halving(terms, own, near_bits, sender):
    for bit in range(near_bits - 1, -1, -1):
        mine_digit = digit_of(own, bit)
        kept = tuple(
            (lax.dynamic_index_in_dim(term, mine_digit, 0, keepdims=False) for term in terms)
        )
        outgoing = tuple(
            (lax.dynamic_index_in_dim(term, 1 - mine_digit, 0, keepdims=False) for term in terms)
        )
        arrived = sender(outgoing, bit)
        terms = tuple((left + right for left, right in zip(kept, arrived)))
    return terms


def log_sigmoid(values):
    return jnp.minimum(values, 0.0) - jnp.log1p(jnp.exp(-jnp.abs(values)))


def flipped(index, bits):
    place = 1
    while place <= bits:
        if bits // place % 2:
            index = index + place * (1 - 2 * (index // place % 2))
        place *= 2
    return index


def step_kernel(
    ways,
    groups,
    seqs,
    tok_hbm,
    gain_hbm,
    wq_hbm,
    wk_hbm,
    wv_hbm,
    wo_hbm,
    wg_hbm,
    bias_hbm,
    head_gain_hbm,
    mix_hbm,
    cell_hbm,
    norm_hbm,
    max_hbm,
    pend_k_hbm,
    pend_v_hbm,
    pend_g_hbm,
    accepted_hbm,
    out,
    cell_new,
    norm_new,
    max_new,
    tok,
    gain,
    weights,
    wg,
    bias,
    head_gain,
    mix_w,
    cell,
    norm,
    stab,
    pend_k,
    pend_v,
    pend_g,
    accepted,
    tok_in,
    scaled,
    wg_in,
    sums,
    part_out,
    part_in,
    fold_rows,
    cell_high,
    cell_low,
    norm_head,
    decay,
    scale_col,
    gated,
    gated_in,
    swap_out,
    swap_in,
    kept,
    answer_out,
    answer_in,
    load_sem,
    tok_send,
    tok_recv,
    fwd_send,
    fwd_recv,
    wg_send,
    wg_recv,
    part_send,
    part_recv,
    gated_send,
    gated_recv,
    swap_send,
    swap_recv,
    answer_send,
    answer_recv,
):
    me = lax.axis_index("kv")
    group = lax.axis_index("tp")
    across, core = group // 2, lax.rem(group, 2)
    side = lax.rem(me, 2)
    count, model_width = tok.shape
    rows = model_width // ways
    half = rows // 2
    chunks, span = weights.shape[0], weights.shape[2] // 4
    heads, head_size = norm.shape[1], norm.shape[2]
    per_chunk = heads // chunks
    proposals = count // seqs
    bits = ways.bit_length() - 1
    f32, bf16 = jnp.float32, jnp.bfloat16
    orders = [tuple(range(bits))] * chunks

    loads = {}

    def load(name, source, target):
        copy = pltpu.make_async_copy(source, target, load_sem.at[len(loads)])
        copy.start()
        loads[name] = copy

    load("tok", tok_hbm, tok)
    load("gain", gain_hbm, gain)
    for chunk in range(chunks):
        for index, source in enumerate((wq_hbm, wk_hbm, wv_hbm, wo_hbm)):
            load(
                ("weight", chunk, index),
                source.at[:, chunk * span : (chunk + 1) * span],
                weights.at[chunk, :, index * span : (index + 1) * span],
            )
    load("wg", wg_hbm, wg)
    load("bias", bias_hbm, bias)
    load("max", max_hbm, stab)
    load("pend_g", pend_g_hbm, pend_g)
    load("accepted", accepted_hbm, accepted)
    load("pend_k", pend_k_hbm, pend_k)
    load("pend_v", pend_v_hbm, pend_v)
    load("norm", norm_hbm, norm)
    load("cell", cell_hbm, cell)
    load("head_gain", head_gain_hbm, head_gain)
    load("mix", mix_hbm, mix_w)

    target = me // 2
    at_home = jnp.logical_and(target == group, core == 0)
    barrier = pltpu.get_barrier_semaphore()

    def signal(where):
        pl.semaphore_signal(
            barrier, inc=1, device_id=where, device_id_type=pl.DeviceIdType.MESH
        )

    partner = {"tp": 2 * across + 1 - core}
    for shift in range(1, ways):
        signal({"kv": flipped(me, shift)})
    signal(partner)
    for which in range(2):
        sender = 2 * group + which
        sender_core = side + which - 2 * side * which
        for other in range(groups // 2):
            sender_group = 2 * other + sender_core

            @pl.when(jnp.logical_or(sender != me, sender_group != group))
            def _():
                signal({"kv": sender, "tp": sender_group})

    @pl.when(at_home)
    def _():
        pl.semaphore_wait(barrier, ways + ways // 2 - 1)

    @pl.when(jnp.logical_not(at_home))
    def _():
        pl.semaphore_wait(barrier, ways + ways // 2)

    sends = []

    def remote(source, target_ref, send_sem, recv_sem, where):
        copy = pltpu.make_async_remote_copy(
            src_ref=source,
            dst_ref=target_ref,
            send_sem=send_sem,
            recv_sem=recv_sem,
            device_id=where,
            device_id_type=pl.DeviceIdType.MESH,
        )
        copy.start()
        sends.append(copy)
        return copy

    def columns(owner):
        return pl.ds(pl.multiple_of(owner * rows, rows), rows)

    halves = pl.ds(pl.multiple_of(core * half, half), half)

    tok_copies, fwd_copies, wg_copies = {}, {}, {}
    loads["tok"].wait()
    whole_first = 1

    def send_tokens(shift):
        there = flipped(me, shift)
        if shift == whole_first:
            source, place = tok.at[:, columns(there)], tok_in.at[shift]
        else:
            source = tok.at[:, pl.ds(pl.multiple_of(there * rows + core * half, half), half)]
            place = tok_in.at[shift, :, halves]
        tok_copies[shift] = remote(
            source, place, tok_send.at[shift], tok_recv.at[shift], {"kv": there}
        )

    first_sends = [shift for shift in range(ways - 1, 1, -1) if shift % 2]
    keepers = [shift for shift in range(ways - 1, 0, -1) if not shift % 2]
    for shift in [whole_first] + first_sends + keepers:
        send_tokens(shift)
    loads["wg"].wait()
    for shift in range(1, ways):
        wg_copies[shift] = remote(
            wg, wg_in.at[shift], wg_send.at[shift], wg_recv.at[shift], {"kv": flipped(me, shift)}
        )

    loads["gain"].wait()
    own_gain = gain[:, columns(me)]

    def scale_block(shift, block):
        scaled[shift] = (block.astype(f32) * own_gain).astype(bf16)

    def forward(shift):
        tok_copies[shift].wait_recv()
        place = tok_in.at[shift, :, halves]
        fwd_copies[shift] = remote(
            place, place, fwd_send.at[shift], fwd_recv.at[shift], partner
        )

    def arrive(shift):
        if shift == whole_first:
            tok_copies[shift].wait_recv()
        else:
            fwd_copies[shift].wait_recv()
        scale_block(shift, tok_in[shift])

    def product(chunk, shift):
        return jnp.dot(scaled[shift], weights[chunk], preferred_element_type=f32)

    part_copies = {}

    def send_part(chunk, shift, bit, value):
        part_out[chunk, shift] = value.astype(bf16)
        part_copies[chunk, shift] = remote(
            part_out.at[chunk, shift],
            part_in.at[chunk, shift],
            part_send.at[chunk, shift],
            part_recv.at[chunk, shift],
            {"kv": flipped(me, 1 << bit)},
        )

    def first_send(chunk, shift):
        send_part(chunk, shift, orders[chunk][0], product(chunk, shift))

    scale_block(0, tok[:, columns(me)])
    squares = jnp.zeros((count, 1), f32)
    for step in range(ways):
        part = tok[:, step * rows : (step + 1) * rows].astype(f32)
        squares = squares + jnp.sum(part * part, axis=1, keepdims=True)
    row_scale = lax.rsqrt(squares / model_width + epsilon)
    scale_col[...] = jnp.broadcast_to(row_scale, scale_col.shape)

    for chunk in range(chunks):
        for index in range(4):
            loads["weight", chunk, index].wait()

    arrive(whole_first)
    for chunk in range(chunks):
        first_send(chunk, whole_first)
    for shift in first_sends:
        forward(shift)

    def eye(size):
        across_rows = lax.broadcasted_iota(jnp.int32, (size, size), 0)
        return across_rows == lax.broadcasted_iota(jnp.int32, (size, size), 1)

    def fold_gates():
        for name in ("bias", "max", "pend_g", "accepted"):
            loads[name].wait()
        bias_col = jnp.sum(
            jnp.where(eye(heads), jnp.broadcast_to(bias[...], (heads, heads)), 0.0),
            axis=1,
            keepdims=True,
        )
        log_in, running = [], []
        total = jnp.zeros((heads, seqs), f32)
        for step in range(proposals):
            taken = jnp.broadcast_to(step < accepted[...], (heads, seqs))
            log_in.append(jnp.where(taken, pend_g[step, 0], very_low))
            total = total + jnp.where(taken, log_sigmoid(pend_g[step, 1] + bias_col), 0.0)
            running.append(total)
        log_w = [total - at + ins for at, ins in zip(running, log_in)]
        carried_log = total + stab[...]
        top = carried_log
        for values in log_w:
            top = jnp.maximum(top, values)
        max_new[...] = top
        fold_rows[...] = jnp.zeros(fold_rows.shape, f32)
        pieces = [jnp.exp(values - top) for values in log_w]
        pieces = pieces + [jnp.exp(carried_log - top), top]
        for index, piece in enumerate(pieces):
            fold_rows[index * heads : (index + 1) * heads, 0:seqs] = piece
        return fold_rows[...].T[:seqs]

    key_scale = head_size ** (-0.5)

    def fold_head(cols, head):
        lanes = slice(head * head_size, (head + 1) * head_size)
        keys = pend_k[:, lanes].astype(f32)
        weighted = []
        carried = jnp.broadcast_to(
            cols[:, proposals * heads + head : proposals * heads + head + 1], (seqs, head_size)
        )
        key_sum = carried * norm[:, head, :]
        for step in range(proposals):
            weight = cols[:, step * heads + head : step * heads + head + 1]
            rows_at = keys[step * seqs : (step + 1) * seqs] * key_scale * weight
            weighted.append(rows_at)
            key_sum = key_sum + rows_at
        norm_head[head] = key_sum
        norm_new[:, head, :] = key_sum
        padding = jnp.zeros((head_size - count, head_size), f32)
        turned = jnp.concatenate(weighted + [padding], axis=0).T
        value_rows = jnp.concatenate(
            [pend_v[:, lanes].astype(f32), padding], axis=0
        ).astype(bf16)
        value_rows = jnp.concatenate([value_rows, value_rows], axis=0)
        high = turned.astype(bf16).astype(f32)
        low = turned - high
        lane = lax.rem(lax.broadcasted_iota(jnp.int32, turned.shape, 1), seqs)
        for seq in range(seqs):
            mine = lane == seq
            left = jnp.concatenate(
                [jnp.where(mine, high, 0.0).astype(bf16), jnp.where(mine, low, 0.0).astype(bf16)],
                axis=1,
            )
            update = jnp.dot(left, value_rows, preferred_element_type=f32)
            result = carried[seq : seq + 1] * cell[seq, head] + update
            cell_new[seq, head] = result
            upper = result.astype(bf16)
            at = slice(seq * head_size, (seq + 1) * head_size)
            cell_high[head, at, :] = upper
            cell_low[head, at, :] = (result - upper.astype(f32)).astype(bf16)

    cols = fold_gates()
    for shift in first_sends:
        arrive(shift)
    for chunk in range(chunks):
        for shift in first_sends:
            first_send(chunk, shift)
    for shift in keepers:
        forward(shift)
    for name in ("pend_k", "pend_v", "norm", "cell"):
        loads[name].wait()
    for head in range(heads):
        fold_head(cols, head)

    for shift in keepers:
        arrive(shift)
    for chunk in range(chunks):
        for shift in keepers + [0]:
            sums[chunk, shift // 2] = product(chunk, shift)

    contract = (((1,), (1,)), ((), ()))
    gates = [jnp.zeros((count, heads), f32)] * 2
    for shift in range(ways):
        owner = flipped(me, shift)
        if shift:
            wg_copies[shift].wait_recv()
            block = (tok[:, columns(owner)].astype(f32) * gain[:, columns(owner)]).astype(bf16)
        else:
            block = scaled[0]
        for part in range(2):
            right = wg_in[shift, part] if shift else wg[part]
            gates[part] = gates[part] + lax.dot_general(
                block, right, contract, preferred_element_type=f32
            )

    def read_gates():
        stabilizer = cols[:, (proposals + 1) * heads : (proposals + 2) * heads]
        log_in, running = [], []
        total = jnp.zeros((seqs, heads), f32)
        scale = scale_col[:, :1]
        gate_in, gate_keep = gates[0] * scale, gates[1] * scale
        index = 0
        for step in range(proposals):
            at = slice(step * seqs, (step + 1) * seqs)
            log_in.append(gate_in[at])
            total = total + log_sigmoid(gate_keep[at] + bias[...])
            running.append(total)
            log_p = total + stabilizer
            log_d = [total - running[past] + log_in[past] for past in range(step + 1)]
            top = log_p
            for values in log_d:
                top = jnp.maximum(top, values)
            for values in log_d + [log_p, None]:
                decay[index, :, :heads] = jnp.exp(-top if values is None else values - top)
                index += 1

    read_gates()

    gated_copies = {}

    def send_gated(chunk, shift, there):
        place = slice(chunk * span, (chunk + 1) * span)
        source = gated.at[:, place]
        gated_copies[chunk, shift] = remote(
            source,
            gated_in.at[shift, :, place],
            gated_send.at[chunk, shift],
            gated_recv.at[chunk, shift],
            {"kv": there},
        )

    def forward_gated(chunk, shift):
        place = slice(chunk * span, (chunk + 1) * span)
        gated_copies[chunk, shift].wait_recv()
        gated_copies[chunk, shift + 1] = remote(
            gated_in.at[shift, :, place],
            gated_in.at[shift + 1, :, place],
            gated_send.at[chunk, shift + 1],
            gated_recv.at[chunk, shift + 1],
            {"kv": flipped(me, 1)},
        )

    def read_head(chunk, local, flat):
        head = chunk * per_chunk + local
        scale = scale_col[...]

        def piece(index):
            at = index * span + local * head_size
            return (flat[:, at : at + head_size] * scale).astype(bf16).astype(f32)

        query, key, value, outgate = (piece(index) for index in range(4))
        key = key * key_scale
        sequence = lax.rem(lax.broadcasted_iota(jnp.int32, query.shape, 0), seqs)
        spread = jnp.concatenate(
            [jnp.where(sequence == seq, query, 0.0).astype(bf16) for seq in range(seqs)], axis=1
        )
        prior = jnp.dot(spread, cell_high[head], preferred_element_type=f32)
        prior = prior + jnp.dot(spread, cell_low[head], preferred_element_type=f32)
        normer = norm_head[head]
        hidden = []
        index = 0
        for step in range(proposals):
            at = slice(step * seqs, (step + 1) * seqs)
            now = query[at]
            numerator, denominator = None, None

            def factor(which):
                return decay[which, :, head : head + 1]

            for past in range(step + 1):
                before = slice(past * seqs, (past + 1) * seqs)
                score = jnp.sum(now * key[before], axis=1, keepdims=True) * factor(index + past)
                term = score * value[before]
                numerator = term if numerator is None else numerator + term
                denominator = score if denominator is None else denominator + score
            prior_w = factor(index + step + 1)
            numerator = numerator + prior_w * prior[at]
            denominator = denominator + prior_w * jnp.sum(now * normer, axis=1, keepdims=True)
            floor = factor(index + step + 2)
            hidden.append(numerator / jnp.maximum(jnp.abs(denominator), floor))
            index += step + 3
        hidden = jnp.concatenate(hidden, axis=0)
        normed = hidden * lax.rsqrt(jnp.mean(hidden * hidden, axis=1, keepdims=True) + epsilon)
        lanes = slice(head * head_size, (head + 1) * head_size)
        normed = normed * head_gain[:, lanes]
        gated[:, lanes] = (jax.nn.sigmoid(outgate) * normed).astype(bf16)

    def take(chunk, stage):
        bit = 1 << orders[chunk][stage]
        done = sum(1 << orders[chunk][early] for early in range(stage + 1))
        later = [1 << b for b in orders[chunk][stage + 1 :]]
        places = [shift for shift in range(ways) if not shift & done]
        places.sort(key=lambda shift: tuple(-(shift // b % 2) for b in later))
        for shift in places:
            part_copies[chunk, shift + bit].wait_recv()
            value = sums[chunk, shift // 2] + part_in[chunk, shift + bit].astype(f32)
            if stage + 1 < bits and shift & later[0]:
                send_part(chunk, shift, orders[chunk][stage + 1], value)
            elif stage + 1 < bits:
                sums[chunk, shift // 2] = value
            else:
                for local in range(per_chunk):
                    read_head(chunk, local, value)

    loads["head_gain"].wait()
    loads["mix"].wait()
    last = chunks - 1
    for tick in range(chunks + bits):
        for stage in range(bits):
            chunk = tick - stage
            if 0 <= chunk < chunks:
                take(chunk, stage)
                if stage == bits - 1:
                    for shift in range(ways - 1, 0, -1):
                        if chunk == last or shift == 1 or not shift % 2:
                            send_gated(chunk, shift, flipped(me, shift))
        chunk = tick - bits
        if 0 <= chunk < last:
            for shift in range(ways - 2, 0, -2):
                forward_gated(chunk, shift)

    def mixed(block):
        return jnp.dot(block, mix_w[...], preferred_element_type=f32)

    swap_copies = {}
    first_core = core == 0
    pairs = list(range(ways // 2 - 1, -1, -1))
    for pair in pairs:
        values = []
        for shift in (2 * pair, 2 * pair + 1):
            if shift:
                for chunk in range(chunks):
                    gated_copies[chunk, shift].wait_recv() if (
                        chunk == last or shift % 2
                    ) else None
                values.append(mixed(gated_in[shift]))
            else:
                values.append(mixed(gated[...]))
        kept[pair] = jnp.where(first_core, values[0], values[1]).astype(bf16)
        swap_out[pair] = jnp.where(first_core, values[1], values[0]).astype(bf16)
        swap_copies[pair] = remote(
            swap_out.at[pair], swap_in.at[pair], swap_send.at[pair], swap_recv.at[pair], partner
        )

    spot = side * (groups // 2) + across

    def answer(pair):
        base = flipped(me, 2 * pair)
        owner = base + core * (1 - 2 * side)
        return pltpu.make_async_remote_copy(
            src_ref=answer_out.at[pair],
            dst_ref=answer_in.at[spot],
            send_sem=answer_send.at[pair],
            recv_sem=answer_recv.at[spot],
            device_id={"kv": owner, "tp": target},
            device_id_type=pl.DeviceIdType.MESH,
        )

    at_own = pltpu.make_async_copy(answer_out.at[0], answer_in.at[spot], answer_recv.at[spot])
    for pair in pairs:
        swap_copies[pair].wait_recv()
        answer_out[pair] = (kept[pair].astype(f32) + swap_in[pair].astype(f32)).astype(bf16)
        if pair:
            copy = answer(pair)
            copy.start()
            sends.append(copy)
        else:

            @pl.when(at_home)
            def _():
                at_own.start()

            @pl.when(jnp.logical_not(at_home))
            def _():
                answer(0).start()

    width = mix_w.shape[1]
    for which in range(2):
        total = None
        for other in range(groups // 2):
            slot = which * (groups // 2) + other
            pltpu.make_async_copy(
                answer_out.at[0], answer_in.at[slot], answer_recv.at[slot]
            ).wait()
            term = answer_in[slot].astype(f32)
            total = term if total is None else total + term
        out[:, which * width : (which + 1) * width] = total.astype(bf16)
    for copy in sends:
        copy.wait_send()

    @pl.when(jnp.logical_not(at_home))
    def _():
        answer(0).wait_send()


def deliver_kernel(*refs):
    sem = refs[-1]
    total = len(refs) // 2
    copies = [
        pltpu.make_async_copy(refs[index], refs[total + index], sem.at[index])
        for index in range(total)
    ]
    for copy in copies:
        copy.start()
    for copy in copies:
        copy.wait()


def one_step(
    tokens,
    norm_gain,
    weights,
    w_gates,
    forget_bias,
    head_gain,
    w_mix,
    state_cell,
    state_norm,
    state_max,
    pend_keys,
    pend_values,
    pend_gates,
    accepted,
):
    ways, groups = lax.axis_size("kv"), lax.axis_size("tp")
    seqs, proposals, model_width = tokens.shape
    count = seqs * proposals
    rows, width = weights[0].shape
    heads, head_size = state_norm.shape[1:]
    chunks = heads
    span = width // chunks
    f32, bf16 = jnp.float32, jnp.bfloat16

    def by_proposal(array):
        return array.transpose(1, 0, 2).reshape(count, array.shape[2])

    operands = (
        by_proposal(tokens),
        norm_gain[None, :],
        *weights,
        w_gates.transpose(1, 2, 0),
        forget_bias[None, :],
        head_gain[None, :],
        w_mix,
        state_cell,
        state_norm,
        state_max.T,
        by_proposal(pend_keys),
        by_proposal(pend_values),
        pend_gates.transpose(1, 2, 3, 0),
        accepted[None, :],
    )
    results = (
        ((count, ways // groups * width), bf16),
        (state_cell.shape, f32),
        (state_norm.shape, f32),
        ((heads, seqs), f32),
    )
    held = [jax.ShapeDtypeStruct(array.shape, array.dtype) for array in operands]
    held = held[:2] + [jax.ShapeDtypeStruct((chunks, rows, 4 * span), bf16)] + held[6:]
    block = (ways, count, rows)
    scratch = [pltpu.VMEM(array.shape, array.dtype) for array in held]
    scratch += [
        pltpu.VMEM(block, bf16),
        pltpu.VMEM(block, bf16),
        pltpu.VMEM((ways, 2, heads, rows), bf16),
        pltpu.VMEM((chunks, ways // 2, count, 4 * span), f32),
        pltpu.VMEM((chunks, ways, count, 4 * span), bf16),
        pltpu.VMEM((chunks, ways, count, 4 * span), bf16),
        pltpu.VMEM(((proposals + 2) * heads, 128), f32),
        pltpu.VMEM((heads, seqs * head_size, head_size), bf16),
        pltpu.VMEM((heads, seqs * head_size, head_size), bf16),
        pltpu.VMEM((heads, seqs, head_size), f32),
        pltpu.VMEM((proposals * (proposals + 5) // 2, seqs, 128), f32),
        pltpu.VMEM((count, head_size), f32),
        pltpu.VMEM((count, width), bf16),
        pltpu.VMEM((ways, count, width), bf16),
    ]
    scratch += [pltpu.VMEM((ways // 2, count, width), bf16)] * 5
    dma = pltpu.SemaphoreType.DMA
    scratch += [dma((len(operands) + 4 * chunks,))]
    scratch += [dma((ways,))] * 6
    scratch += [dma((chunks, ways))] * 4
    scratch += [dma((ways,))] * 4
    hbm = pltpu.MemorySpace.HBM
    anywhere = pl.BlockSpec(memory_space=hbm)
    vmem = pl.BlockSpec(memory_space=pltpu.VMEM)
    held = pl.pallas_call(
        functools.partial(step_kernel, ways, groups, seqs),
        out_shape=tuple(pltpu.VMEM(shape, dtype) for shape, dtype in results),
        in_specs=[anywhere] * len(operands),
        out_specs=(vmem,) * len(results),
        scratch_shapes=scratch,
        compiler_params=pltpu.CompilerParams(
            collective_id=0, has_side_effects=True, vmem_limit_bytes=40 * 2**20
        ),
    )(*(pltpu.with_memory_space_constraint(array, hbm) for array in operands))
    mixed_out, cell_new, norm_new, max_new = pl.pallas_call(
        deliver_kernel,
        out_shape=tuple(jax.ShapeDtypeStruct(shape, dtype) for shape, dtype in results),
        in_specs=[vmem] * len(results),
        out_specs=(anywhere,) * len(results),
        scratch_shapes=[dma((len(results),))],
    )(*(pltpu.with_memory_space_constraint(array, pltpu.VMEM) for array in held))
    mixed_out = mixed_out.reshape(proposals, seqs, -1).transpose(1, 0, 2)
    return mixed_out, cell_new, norm_new, max_new.T


def project_by_digits(flat_rows, norm_gain, weights, w_mix):
    token_count, model_width = flat_rows.shape
    shard_rows = weights[0].shape[0]
    own = lax.axis_index("kv")
    kv_bits = lax.axis_size("kv").bit_length() - 1
    near_bits = kv_bits // 2
    near = 2**near_bits
    far = lax.axis_size("kv") // near
    digit_shape = (2,) * near_bits
    collected = collect_digits(
        weights + (w_mix,),
        (0, 0, 0, 0, 0, 1),
        own,
        range(near_bits, kv_bits),
        lambda parts, bit: jax.tree.map(
            lambda part, own: part.astype(own.dtype),
            from_partner(shortened(parts), "kv", bit),
            parts,
        ),
    )
    far_mix = collected[5]
    token_digits = jnp.moveaxis(flat_rows.reshape(token_count, far, near, shard_rows), 2, 0)
    token_digits = token_digits.reshape(digit_shape + (token_count, far, shard_rows))
    arrived = butterfly(
        token_digits, own, near_bits, lambda part, bit: from_partner(part, "kv", bit)
    )
    gathered = arrived.reshape(near * token_count, far * shard_rows)
    gain_part = lax.dynamic_index_in_dim(
        norm_gain.reshape(far, near, shard_rows), own % near, 1, keepdims=False
    ).reshape(far * shard_rows)
    widened = gathered.astype(jnp.float32)
    scaled_in = (widened * gain_part).astype(jnp.bfloat16)
    partials = tuple(
        (
            jnp.dot(scaled_in, weight, preferred_element_type=jnp.float32).reshape(
                digit_shape + (token_count, weight.shape[1])
            )
            for weight in collected[:5]
        )
    )
    part_squares = jnp.sum(widened * widened, axis=-1).reshape(digit_shape + (token_count,))
    summed = halving(
        partials + (part_squares,),
        own,
        near_bits,
        lambda parts, bit: jax.tree.map(
            lambda part, own: part.astype(own.dtype),
            from_partner(shortened(parts), "kv", bit),
            parts,
        ),
    )
    totals = summed[:5]
    sum_squares = summed[5]
    row_scale = lax.rsqrt(sum_squares / model_width + epsilon)[:, None]
    return (
        tuple((total * row_scale).astype(jnp.bfloat16) for total in totals[:4]),
        totals[4] * row_scale,
        far_mix,
    )


def mix_by_digits(gated_rows, far_mix, model_width):
    token_count = gated_rows.shape[0]
    shard_rows = model_width // lax.axis_size("kv")
    own = lax.axis_index("kv")
    kv_bits = lax.axis_size("kv").bit_length() - 1
    near_bits = kv_bits // 2
    near = 2**near_bits
    far = lax.axis_size("kv") // near
    digit_shape = (2,) * near_bits
    near_gated = collect_digits(
        (gated_rows,),
        (0,),
        own,
        range(near_bits),
        lambda parts, bit: jax.tree.map(
            lambda part, own: part.astype(own.dtype),
            from_partner(shortened(parts), "kv", bit),
            parts,
        ),
    )[0]
    group_part = jnp.dot(near_gated, far_mix, preferred_element_type=jnp.float32).astype(
        jnp.bfloat16
    )
    group_part = group_part.reshape(digit_shape + (token_count, far, shard_rows))
    placed = butterfly(group_part, own, near_bits, lambda part, bit: from_partner(part, "kv", bit))
    placed = placed.reshape(near, token_count, far, shard_rows).transpose(1, 2, 0, 3)
    partial_out = placed.reshape(token_count, model_width).astype(jnp.float32)
    mixed_out = lax.psum_scatter(
        partial_out.astype(jnp.bfloat16), "tp", scatter_dimension=1, tiled=True
    )
    return mixed_out


def shards(
    tokens,
    norm_gain,
    w_query,
    w_key,
    w_value,
    w_outgate,
    w_gates,
    forget_bias,
    head_gain,
    w_mix,
    state_cell,
    state_norm,
    state_max,
    pend_keys,
    pend_values,
    pend_gates,
    accepted,
):
    sequences, proposals, model_width = tokens.shape
    token_count = sequences * proposals
    local_heads = forget_bias.shape[0]
    head_size = state_cell.shape[-1]
    shard_rows = w_query.shape[0]
    weights = (w_query, w_key, w_value, w_outgate)
    ways, groups = lax.axis_size("kv"), lax.axis_size("tp")
    direct = (
        shard_rows % 256 == 0
        and w_mix.shape[1] == shard_rows
        and w_query.shape[1] == shard_rows
        and ways == 2 * groups
        and groups % 2 == 0
        and sequences == 8
        and head_size == 128
        and token_count <= head_size
    )
    if direct:
        return one_step(
            tokens,
            norm_gain,
            weights,
            w_gates,
            forget_bias,
            head_gain,
            w_mix,
            state_cell,
            state_norm,
            state_max,
            pend_keys,
            pend_values,
            pend_gates,
            accepted,
        )
    flat_gates = w_gates.reshape(shard_rows, -1)
    flat_rows = tokens.reshape(token_count, model_width)
    projected, gate_pre, far_mix = project_by_digits(
        flat_rows, norm_gain, weights + (flat_gates,), w_mix
    )
    queries, new_keys, new_values, outgate = projected
    gate_pre = gate_pre.reshape(sequences, proposals, 2, local_heads)

    def split_heads(array):
        return array.astype(jnp.float32).reshape(sequences, proposals, local_heads, head_size)

    key_scale = head_size ** (-0.5)
    cell_new, norm_new, new_max = fold_pending(
        state_cell,
        state_norm,
        state_max,
        split_heads(pend_keys) * key_scale,
        split_heads(pend_values),
        pend_gates,
        forget_bias,
        accepted,
    )
    log_in = gate_pre[:, :, 0, :]
    log_keep = jax.nn.log_sigmoid(gate_pre[:, :, 1, :] + forget_bias)
    hidden = read_block(
        split_heads(queries),
        split_heads(new_keys) * key_scale,
        split_heads(new_values),
        log_in,
        log_keep,
        cell_new,
        norm_new,
        new_max,
    )
    normed = hidden * lax.rsqrt(jnp.mean(hidden * hidden, axis=-1, keepdims=True) + epsilon)
    normed = normed * head_gain.reshape(local_heads, head_size)
    gated_rows = (jax.nn.sigmoid(split_heads(outgate)) * normed).astype(jnp.bfloat16)
    gated_rows = gated_rows.reshape(token_count, local_heads * head_size)
    mixed_out = mix_by_digits(gated_rows, far_mix, model_width)
    return (mixed_out.reshape(sequences, proposals, -1), cell_new, norm_new, new_max)


def solution(mesh):
    return jax.shard_map(
        shards,
        mesh=mesh,
        in_specs=(
            P("kv", None, None),
            P(),
            P("kv", "tp"),
            P("kv", "tp"),
            P("kv", "tp"),
            P("kv", "tp"),
            P("kv", None, "tp"),
            P("tp"),
            P("tp"),
            P("tp", "kv"),
            P("kv", "tp", None, None),
            P("kv", "tp", None),
            P("kv", "tp"),
            P("kv", None, "tp"),
            P("kv", None, "tp"),
            P("kv", None, None, "tp"),
            P("kv"),
        ),
        out_specs=(
            P("kv", None, "tp"),
            P("kv", "tp", None, None),
            P("kv", "tp", None),
            P("kv", "tp"),
        ),
        check_vma=False,
    )
```

```python
import functools

import jax
import jax.numpy as jnp
from jax import lax
from jax.experimental import pallas as pl
from jax.experimental.pallas import tpu as pltpu
from jax.sharding import PartitionSpec as P

epsilon = 1e-06
very_low = -1e30
highest = lax.Precision.HIGHEST


def shortened(shard):

    def short(part):
        return part.astype(jnp.bfloat16) if part.dtype == jnp.float32 else part

    return jax.tree.map(short, shard)


def from_partner(shard, axis, stride):
    return lax.ppermute(shard, axis, [(i, i ^ 1 << stride) for i in range(lax.axis_size(axis))])


def running_sum(values):
    steps = values.shape[1]
    upto = jnp.arange(steps)[:, None] >= jnp.arange(steps)[None, :]
    return jnp.sum(jnp.where(upto[None, :, :, None], values[:, None], 0.0), axis=2)


def fold_pending(
    cell_state, normer, stabilizer, key_rows, value_rows, gate_rows, forget_shift, accepted
):
    proposals = key_rows.shape[1]
    accepted_mask = jnp.arange(proposals)[None, :, None] < accepted[:, None, None]
    log_in = jnp.where(accepted_mask, gate_rows[:, :, 0, :], very_low)
    log_keep = jnp.where(
        accepted_mask, jax.nn.log_sigmoid(gate_rows[:, :, 1, :] + forget_shift), 0.0
    )
    running = running_sum(log_keep)
    block_total = running[:, -1]
    log_w = block_total[:, None, :] - running + log_in
    new_max = jnp.maximum(block_total + stabilizer, jnp.max(log_w, axis=1))
    weights = jnp.exp(log_w - new_max[:, None, :])
    carried = jnp.exp(block_total + stabilizer - new_max)
    weighted_keys = weights[..., None] * key_rows
    cell_new = carried[..., None, None] * cell_state + jnp.einsum(
        "sphd,sphe->shde", weighted_keys, value_rows, precision=highest
    )
    norm_new = carried[..., None] * normer + jnp.sum(weighted_keys, axis=1)
    return (cell_new, norm_new, new_max)


def read_block(queries, key_rows, value_rows, log_in, log_keep, cell_state, normer, stabilizer):
    proposals = queries.shape[1]
    causal = jnp.arange(proposals)[:, None] >= jnp.arange(proposals)[None, :]
    running_h = jnp.moveaxis(running_sum(log_keep), 1, 2)
    input_h = jnp.moveaxis(log_in, 1, 2)
    log_d = jnp.where(
        causal, running_h[..., :, None] - running_h[..., None, :] + input_h[..., None, :], very_low
    )
    log_p = running_h + stabilizer[..., None]
    top_log = jnp.maximum(log_p, jnp.max(log_d, axis=-1))
    decays = jnp.exp(log_d - top_log[..., None])
    prior_w = jnp.exp(log_p - top_log)
    scores = jnp.einsum("sthd,suhd->shtu", queries, key_rows, precision=highest) * decays
    numerator = jnp.einsum("shtu,suhe->shte", scores, value_rows, precision=highest)
    numerator = numerator + prior_w[..., None] * jnp.einsum(
        "sthd,shde->shte", queries, cell_state, precision=highest
    )
    denominator = jnp.sum(scores, axis=-1) + prior_w * jnp.einsum(
        "sthd,shd->sht", queries, normer, precision=highest
    )
    hidden_out = numerator / jnp.maximum(jnp.abs(denominator), jnp.exp(-top_log))[..., None]
    return jnp.moveaxis(hidden_out, 1, 2)


def digit_of(own, bit):
    return own // 2**bit % 2


def collect_digits(pieces, dims, own, bits, sender):
    for bit in bits:
        others = sender(pieces, bit)
        first = digit_of(own, bit) == 0
        pieces = tuple(
            (
                jnp.where(
                    first,
                    jnp.concatenate((mine, theirs), axis=dim),
                    jnp.concatenate((theirs, mine), axis=dim),
                )
                for mine, theirs, dim in zip(pieces, others, dims)
            )
        )
    return pieces


def butterfly(blocks, own, near_bits, sender):
    for bit in range(near_bits):
        axis = near_bits - 1 - bit
        mine_digit = digit_of(own, bit)
        kept = lax.dynamic_index_in_dim(blocks, mine_digit, axis, keepdims=False)
        outgoing = lax.dynamic_index_in_dim(blocks, 1 - mine_digit, axis, keepdims=False)
        arrived = sender(outgoing, bit)
        blocks = jnp.where(
            mine_digit == 0,
            jnp.stack((kept, arrived), axis=axis),
            jnp.stack((arrived, kept), axis=axis),
        )
    return blocks


def halving(terms, own, near_bits, sender):
    for bit in range(near_bits - 1, -1, -1):
        mine_digit = digit_of(own, bit)
        kept = tuple(
            (lax.dynamic_index_in_dim(term, mine_digit, 0, keepdims=False) for term in terms)
        )
        outgoing = tuple(
            (lax.dynamic_index_in_dim(term, 1 - mine_digit, 0, keepdims=False) for term in terms)
        )
        arrived = sender(outgoing, bit)
        terms = tuple((left + right for left, right in zip(kept, arrived)))
    return terms


def log_sigmoid(values):
    return jnp.minimum(values, 0.0) - jnp.log1p(jnp.exp(-jnp.abs(values)))


def flipped(index, bits):
    place = 1
    while place <= bits:
        if bits // place % 2:
            index = index + place * (1 - 2 * (index // place % 2))
        place *= 2
    return index


spread_chunks = (3,)
tasks = (('forward', 3), ('forward', 6), ('gate fold', 0), ('forward', 5), ('forward', 4), ('forward', 7), ('weights', 0), ('arrive', 3), ('send', (3, 0)), ('send', (3, 1)), ('arrive', 6), ('send', (6, 0)), ('arrive', 5), ('send', (5, 1)), ('arrive', 7), ('send', (7, 0)), ('send', (7, 1)), ('send', (7, 2)), ('send', (3, 2)), ('send', (5, 2)), ('send', (7, 3)), ('send', (3, 3)), ('send', (5, 3)), ('arrive', 4), ('sums', 0), ('fold', 0), ('fold', 1), ('fold', 2), ('fold', 3), (0, 0), ('sums', 1), (0, 1), (1, 0), ('sums', 2), (0, 2), (1, 1), ('squares', 0), ('gates', 0), ('sums', 3), (2, 0), (1, 2), (0, 3), (2, 1), ('pass', 0), (2, 2), ('pass', 1), (1, 3), ('pass', 2),
)


def step_kernel(
    ways,
    groups,
    seqs,
    tok_hbm,
    gain_hbm,
    wq_hbm,
    wk_hbm,
    wv_hbm,
    wo_hbm,
    wg_hbm,
    bias_hbm,
    head_gain_hbm,
    mix_hbm,
    cell_hbm,
    norm_hbm,
    max_hbm,
    pend_k_hbm,
    pend_v_hbm,
    pend_g_hbm,
    accepted_hbm,
    out,
    cell_new,
    norm_new,
    max_new,
    tok,
    gain,
    weights,
    wg,
    bias,
    head_gain,
    mix_w,
    cell,
    norm,
    stab,
    pend_k,
    pend_v,
    pend_g,
    accepted,
    tok_in,
    scaled,
    wg_in,
    sums,
    part_out,
    part_in,
    fold_rows,
    cell_high,
    cell_low,
    norm_head,
    decay,
    scale_col,
    gated,
    gated_in,
    answer_out,
    answer_in,
    load_sem,
    tok_send,
    tok_recv,
    fwd_send,
    fwd_recv,
    wg_send,
    wg_recv,
    part_send,
    part_recv,
    gated_send,
    gated_recv,
    pass_send,
    mix_send,
    mix_recv,
    answer_send,
    answer_recv,
):
    me = lax.axis_index("kv")
    group = lax.axis_index("tp")
    across, core = group // 2, lax.rem(group, 2)
    side = lax.rem(me, 2)
    count, model_width = tok.shape
    rows = model_width // ways
    half = rows // 2
    chunks, span = weights.shape[0], weights.shape[2] // 4
    heads, head_size = norm.shape[1], norm.shape[2]
    per_chunk = heads // chunks
    proposals = count // seqs
    bits = ways.bit_length() - 1
    f32, bf16 = jnp.float32, jnp.bfloat16
    near_first = tuple(range(bits))
    far_first = near_first[1:] + near_first[:1]
    plans = [(near_first, False)] * chunks
    plans[0] = (far_first, False)
    plans[-1] = (near_first, True)

    def first_bit(chunk):
        return 1 << plans[chunk][0][0]

    def slot(chunk, shift):
        return sum(1 for other in range(shift) if not other & first_bit(chunk))


    loads = {}

    def load(name, source, target):
        copy = pltpu.make_async_copy(source, target, load_sem.at[len(loads)])
        copy.start()
        loads[name] = copy

    load("tok", tok_hbm, tok)
    load("gain", gain_hbm, gain)
    for chunk in range(chunks):
        for index, source in enumerate((wq_hbm, wk_hbm, wv_hbm, wo_hbm)):
            load(
                ("weight", chunk, index),
                source.at[:, chunk * span : (chunk + 1) * span],
                weights.at[chunk, :, index * span : (index + 1) * span],
            )
    load("wg", wg_hbm, wg)
    load("bias", bias_hbm, bias)
    load("max", max_hbm, stab)
    load("pend_g", pend_g_hbm, pend_g)
    load("accepted", accepted_hbm, accepted)
    load("pend_k", pend_k_hbm, pend_k)
    load("pend_v", pend_v_hbm, pend_v)
    load("norm", norm_hbm, norm)
    load("cell", cell_hbm, cell)
    load("head_gain", head_gain_hbm, head_gain)
    load("mix", mix_hbm, mix_w.at[core])

    target = me // 2
    at_home = jnp.logical_and(target == group, core == 0)
    barrier = pltpu.get_barrier_semaphore()

    def signal(where):
        pl.semaphore_signal(
            barrier, inc=1, device_id=where, device_id_type=pl.DeviceIdType.MESH
        )

    partner = {"tp": 2 * across + 1 - core}
    for shift in range(1, ways):
        for other in range(2):
            signal({"kv": flipped(me, shift), "tp": 2 * across + other})
    signal(partner)
    for which in range(2):
        sender = 2 * group + which
        sender_core = side + which - 2 * side * which
        for other in range(groups // 2):
            sender_group = 2 * other + sender_core

            @pl.when(jnp.logical_or(sender != me, sender_group != group))
            def _():
                signal({"kv": sender, "tp": sender_group})

    greetings = 2 * (ways - 1) + 1 + ways // 2

    @pl.when(at_home)
    def _():
        pl.semaphore_wait(barrier, greetings - 1)

    @pl.when(jnp.logical_not(at_home))
    def _():
        pl.semaphore_wait(barrier, greetings)

    sends = []

    def remote(source, target_ref, send_sem, recv_sem, where):
        copy = pltpu.make_async_remote_copy(
            src_ref=source,
            dst_ref=target_ref,
            send_sem=send_sem,
            recv_sem=recv_sem,
            device_id=where,
            device_id_type=pl.DeviceIdType.MESH,
        )
        copy.start()
        sends.append(copy)
        return copy

    def columns(owner):
        return pl.ds(pl.multiple_of(owner * rows, rows), rows)

    halves = pl.ds(pl.multiple_of(core * half, half), half)

    tok_copies, fwd_copies, wg_copies = {}, {}, {}
    loads["tok"].wait()
    whole = (1, 2)

    def send_tokens(shift):
        there = flipped(me, shift)
        if shift in whole:
            source, place = tok.at[:, columns(there)], tok_in.at[shift]
        else:
            source = tok.at[:, pl.ds(pl.multiple_of(there * rows + core * half, half), half)]
            place = tok_in.at[shift, :, halves]
        tok_copies[shift] = remote(
            source, place, tok_send.at[shift], tok_recv.at[shift], {"kv": there}
        )

    others = [shift for shift in (7, 3, 6, 5, 4) if shift < ways]
    for shift in list(whole) + others:
        send_tokens(shift)

    loads["gain"].wait()
    own_gain = gain[:, columns(me)]

    def scale_block(shift, block):
        scaled[shift] = (block.astype(f32) * own_gain).astype(bf16)

    def forward(shift):
        tok_copies[shift].wait_recv()
        place = tok_in.at[shift, :, halves]
        fwd_copies[shift] = remote(
            place, place, fwd_send.at[shift], fwd_recv.at[shift], partner
        )

    def arrive(shift):
        if shift in whole:
            tok_copies[shift].wait_recv()
        else:
            fwd_copies[shift].wait_recv()
        scale_block(shift, tok_in[shift])

    def product(chunk, shift):
        return jnp.dot(scaled[shift], weights[chunk], preferred_element_type=f32)

    part_copies = {}
    mix_copy = []

    def send_part(chunk, shift, move, value):
        part_out[chunk, shift] = value.astype(bf16)
        part_copies[chunk, shift] = remote(
            part_out.at[chunk, shift],
            part_in.at[chunk, shift],
            part_send.at[chunk, shift],
            part_recv.at[chunk, shift],
            {"kv": flipped(me, move)},
        )

    def first_send(shift, some):
        for chunk in some:
            if shift & first_bit(chunk):
                send_part(chunk, shift, first_bit(chunk), product(chunk, shift))

    scale_block(0, tok[:, columns(me)])
    for chunk in range(chunks):
        for index in range(4):
            loads["weight", chunk, index].wait()

    every = range(chunks)
    for shift in whole:
        arrive(shift)
        first_send(shift, every)
    def send_gates():
        loads["mix"].wait()
        mix_copy.append(remote(mix_w.at[core], mix_w.at[core], mix_send, mix_recv, partner))
        loads["wg"].wait()
        for shift in range(1, ways):
            wg_copies[shift] = remote(
                wg,
                wg_in.at[shift],
                wg_send.at[shift],
                wg_recv.at[shift],
                {"kv": flipped(me, shift)},
            )

    def square_rows():
        squares = jnp.zeros((count, 1), f32)
        for step in range(ways):
            part = tok[:, step * rows : (step + 1) * rows].astype(f32)
            squares = squares + jnp.sum(part * part, axis=1, keepdims=True)
        row_scale = lax.rsqrt(squares / model_width + epsilon)
        scale_col[...] = jnp.broadcast_to(row_scale, scale_col.shape)

    def eye(size):
        across_rows = lax.broadcasted_iota(jnp.int32, (size, size), 0)
        return across_rows == lax.broadcasted_iota(jnp.int32, (size, size), 1)

    def fold_gates():
        for name in ("bias", "max", "pend_g", "accepted"):
            loads[name].wait()
        bias_col = jnp.sum(
            jnp.where(eye(heads), jnp.broadcast_to(bias[...], (heads, heads)), 0.0),
            axis=1,
            keepdims=True,
        )
        log_in, running = [], []
        total = jnp.zeros((heads, seqs), f32)
        for step in range(proposals):
            taken = jnp.broadcast_to(step < accepted[...], (heads, seqs))
            log_in.append(jnp.where(taken, pend_g[step, 0], very_low))
            total = total + jnp.where(taken, log_sigmoid(pend_g[step, 1] + bias_col), 0.0)
            running.append(total)
        log_w = [total - at + ins for at, ins in zip(running, log_in)]
        carried_log = total + stab[...]
        top = carried_log
        for values in log_w:
            top = jnp.maximum(top, values)
        max_new[...] = top
        fold_rows[...] = jnp.zeros(fold_rows.shape, f32)
        pieces = [jnp.exp(values - top) for values in log_w]
        pieces = pieces + [jnp.exp(carried_log - top), top]
        for index, piece in enumerate(pieces):
            fold_rows[index * heads : (index + 1) * heads, 0:seqs] = piece
        return fold_rows[...].T[:seqs]

    key_scale = head_size ** (-0.5)

    def fold_head(cols, head):
        lanes = slice(head * head_size, (head + 1) * head_size)
        keys = pend_k[:, lanes].astype(f32)
        weighted = []
        carried = jnp.broadcast_to(
            cols[:, proposals * heads + head : proposals * heads + head + 1], (seqs, head_size)
        )
        key_sum = carried * norm[:, head, :]
        for step in range(proposals):
            weight = cols[:, step * heads + head : step * heads + head + 1]
            rows_at = keys[step * seqs : (step + 1) * seqs] * key_scale * weight
            weighted.append(rows_at)
            key_sum = key_sum + rows_at
        norm_head[head] = key_sum
        norm_new[:, head, :] = key_sum
        padding = jnp.zeros((head_size - count, head_size), f32)
        turned = jnp.concatenate(weighted + [padding], axis=0).T
        value_rows = jnp.concatenate(
            [pend_v[:, lanes].astype(f32), padding], axis=0
        ).astype(bf16)
        value_rows = jnp.concatenate([value_rows, value_rows], axis=0)
        high = turned.astype(bf16).astype(f32)
        low = turned - high
        lane = lax.rem(lax.broadcasted_iota(jnp.int32, turned.shape, 1), seqs)
        for seq in range(seqs):
            mine = lane == seq
            left = jnp.concatenate(
                [jnp.where(mine, high, 0.0).astype(bf16), jnp.where(mine, low, 0.0).astype(bf16)],
                axis=1,
            )
            update = jnp.dot(left, value_rows, preferred_element_type=f32)
            result = carried[seq : seq + 1] * cell[seq, head] + update
            cell_new[seq, head] = result
            upper = result.astype(bf16)
            at = slice(seq * head_size, (seq + 1) * head_size)
            cell_high[head, at, :] = upper
            cell_low[head, at, :] = (result - upper.astype(f32)).astype(bf16)

    cols = []

    def own_sums(chunk):
        for shift in range(ways):
            if not shift & first_bit(chunk):
                sums[chunk, slot(chunk, shift)] = product(chunk, shift)

    contract = (((1,), (1,)), ((), ()))

    def read_gates():
        gates = [jnp.zeros((count, heads), f32)] * 2
        for shift in range(ways):
            owner = flipped(me, shift)
            if shift:
                wg_copies[shift].wait_recv()
                block = (tok[:, columns(owner)].astype(f32) * gain[:, columns(owner)]).astype(bf16)
            else:
                block = scaled[0]
            for part in range(2):
                right = wg_in[shift, part] if shift else wg[part]
                gates[part] = gates[part] + lax.dot_general(
                    block, right, contract, preferred_element_type=f32
                )
        stabilizer = cols[0][:, (proposals + 1) * heads : (proposals + 2) * heads]
        log_in, running = [], []
        total = jnp.zeros((seqs, heads), f32)
        scale = scale_col[:, :1]
        gate_in, gate_keep = gates[0] * scale, gates[1] * scale
        index = 0
        for step in range(proposals):
            at = slice(step * seqs, (step + 1) * seqs)
            log_in.append(gate_in[at])
            total = total + log_sigmoid(gate_keep[at] + bias[...])
            running.append(total)
            log_p = total + stabilizer
            log_d = [total - running[past] + log_in[past] for past in range(step + 1)]
            top = log_p
            for values in log_d:
                top = jnp.maximum(top, values)
            for values in log_d + [log_p, None]:
                decay[index, :, :heads] = jnp.exp(-top if values is None else values - top)
                index += 1

    first_core, second_core = core == 0, core == 1

    def gated_copy(chunk, source, pair, origin, send_sem, there, there_core):
        place = slice(chunk * span, (chunk + 1) * span)
        return pltpu.make_async_remote_copy(
            src_ref=source.at[:, place],
            dst_ref=gated_in.at[pair, origin, :, place],
            send_sem=send_sem,
            recv_sem=gated_recv.at[chunk, 2 * pair + origin],
            device_id={"kv": there, "tp": 2 * across + there_core},
            device_id_type=pl.DeviceIdType.MESH,
        )

    def to_own_chip(chunk):
        return gated_copy(chunk, gated, 0, core, gated_send.at[chunk, 0], me, 0)

    def arrived(chunk, pair, origin):
        place = slice(chunk * span, (chunk + 1) * span)
        pltpu.make_async_copy(
            gated.at[:, place],
            gated_in.at[pair, origin, :, place],
            gated_recv.at[chunk, 2 * pair + origin],
        ).wait()

    def passed(chunk, pair, origin):
        return gated_copy(
            chunk,
            gated_in.at[pair, origin],
            pair,
            origin,
            pass_send.at[chunk, 2 * pair + origin],
            flipped(me, 1),
            1,
        )

    def send_gated(chunk):
        for shift in range(ways - 1, 0, -1):
            if chunk in spread_chunks or shift == 1 or not shift % 2:
                copy = gated_copy(
                    chunk,
                    gated,
                    shift // 2,
                    core,
                    gated_send.at[chunk, shift],
                    flipped(me, shift),
                    shift % 2,
                )
                copy.start()
                sends.append(copy)

        @pl.when(second_core)
        def _():
            to_own_chip(chunk).start()

        @pl.when(first_core)
        def _():
            place = slice(chunk * span, (chunk + 1) * span)
            pltpu.make_async_copy(
                gated.at[:, place], gated_in.at[0, 0, :, place], gated_recv.at[chunk, 0]
            ).start()

    def pass_gated(chunk):
        @pl.when(first_core)
        def _():
            for pair in range(ways // 2 - 1, 0, -1):
                for origin in range(2):
                    arrived(chunk, pair, origin)
                    passed(chunk, pair, origin).start()

    def read_head(chunk, local, flat):
        head = chunk * per_chunk + local
        scale = scale_col[...]

        def piece(index):
            at = index * span + local * head_size
            return (flat[:, at : at + head_size] * scale).astype(bf16).astype(f32)

        query, key, value, outgate = (piece(index) for index in range(4))
        key = key * key_scale
        sequence = lax.rem(lax.broadcasted_iota(jnp.int32, query.shape, 0), seqs)
        spread = jnp.concatenate(
            [jnp.where(sequence == seq, query, 0.0).astype(bf16) for seq in range(seqs)], axis=1
        )
        prior = jnp.dot(spread, cell_high[head], preferred_element_type=f32)
        prior = prior + jnp.dot(spread, cell_low[head], preferred_element_type=f32)
        normer = norm_head[head]
        hidden = []
        index = 0
        for step in range(proposals):
            at = slice(step * seqs, (step + 1) * seqs)
            now = query[at]
            numerator, denominator = None, None

            def factor(which):
                return decay[which, :, head : head + 1]

            for past in range(step + 1):
                before = slice(past * seqs, (past + 1) * seqs)
                score = jnp.sum(now * key[before], axis=1, keepdims=True) * factor(index + past)
                term = score * value[before]
                numerator = term if numerator is None else numerator + term
                denominator = score if denominator is None else denominator + score
            prior_w = factor(index + step + 1)
            numerator = numerator + prior_w * prior[at]
            denominator = denominator + prior_w * jnp.sum(now * normer, axis=1, keepdims=True)
            floor = factor(index + step + 2)
            hidden.append(numerator / jnp.maximum(jnp.abs(denominator), floor))
            index += step + 3
        hidden = jnp.concatenate(hidden, axis=0)
        normed = hidden * lax.rsqrt(jnp.mean(hidden * hidden, axis=1, keepdims=True) + epsilon)
        lanes = slice(head * head_size, (head + 1) * head_size)
        normed = normed * head_gain[:, lanes]
        gated[:, lanes] = (jax.nn.sigmoid(outgate) * normed).astype(bf16)

    def complete(chunk, value):
        for local in range(per_chunk):
            read_head(chunk, local, value)
        send_gated(chunk)

    def take(chunk, stage):
        order, straight = plans[chunk]
        if straight and stage:
            value = sums[chunk, 0]
            for shift in range(1, ways):
                if not shift & first_bit(chunk):
                    part_copies[chunk, shift].wait_recv()
                    value = value + part_in[chunk, shift].astype(f32)
            complete(chunk, value)
            return
        bit = 1 << order[stage]
        done = sum(1 << b for b in order[: stage + 1])
        later = [1 << b for b in order[stage + 1 :]]
        places = [shift for shift in range(ways) if not shift & done]
        places.sort(key=lambda shift: tuple(-(shift // b % 2) for b in later))
        for shift in places:
            part_copies[chunk, shift + bit].wait_recv()
            value = sums[chunk, slot(chunk, shift)] + part_in[chunk, shift + bit].astype(f32)
            if straight and shift:
                send_part(chunk, shift, shift, value)
            elif later and shift & later[0]:
                send_part(chunk, shift, later[0], value)
            elif later:
                sums[chunk, slot(chunk, shift)] = value
            else:
                complete(chunk, value)

    for kind, which in tasks:
        if kind == "forward":
            forward(which)
        elif kind == "arrive":
            arrive(which)
        elif kind == "send":
            first_send(which[0], [which[1]])
        elif kind == "sums":
            own_sums(which)
        elif kind == "gate fold":
            cols.append(fold_gates())
        elif kind == "fold":
            if not which:
                for name in ("pend_k", "pend_v", "norm", "cell"):
                    loads[name].wait()
            fold_head(cols[0], which)
        elif kind == "weights":
            send_gates()
        elif kind == "squares":
            square_rows()
        elif kind == "gates":
            loads["head_gain"].wait()
            read_gates()
        elif kind == "pass":
            pass_gated(which)
        else:
            take(which, kind)

    spot = side * (groups // 2) + across

    def answer(pair):
        base = flipped(me, 2 * pair)
        owner = base + core * (1 - 2 * side)
        return pltpu.make_async_remote_copy(
            src_ref=answer_out.at[pair],
            dst_ref=answer_in.at[spot],
            send_sem=answer_send.at[pair],
            recv_sem=answer_recv.at[spot],
            device_id={"kv": owner, "tp": target},
            device_id_type=pl.DeviceIdType.MESH,
        )

    at_own = pltpu.make_async_copy(answer_out.at[0], answer_in.at[spot], answer_recv.at[spot])
    mix_copy[0].wait_recv()
    for pair in range(ways // 2):
        for chunk in range(chunks):
            for origin in range(2):
                if chunk in spread_chunks or not pair:
                    arrived(chunk, pair, origin)
        for chunk in range(chunks):
            if chunk not in spread_chunks and pair:

                @pl.when(second_core)
                def _():
                    for origin in range(2):
                        arrived(chunk, pair, origin)

        value = jnp.dot(gated_in[pair, 0], mix_w[0], preferred_element_type=f32)
        value = value + jnp.dot(gated_in[pair, 1], mix_w[1], preferred_element_type=f32)
        answer_out[pair] = value.astype(bf16)
        if pair:
            copy = answer(pair)
            copy.start()
            sends.append(copy)
        else:

            @pl.when(at_home)
            def _():
                at_own.start()

            @pl.when(jnp.logical_not(at_home))
            def _():
                answer(0).start()

    width = mix_w.shape[2]
    for which in range(2):
        total = None
        for other in range(groups // 2):
            slot = which * (groups // 2) + other
            pltpu.make_async_copy(
                answer_out.at[0], answer_in.at[slot], answer_recv.at[slot]
            ).wait()
            term = answer_in[slot].astype(f32)
            total = term if total is None else total + term
        out[:, which * width : (which + 1) * width] = total.astype(bf16)
    for copy in sends:
        copy.wait_send()

    @pl.when(second_core)
    def _():
        for chunk in range(chunks):
            to_own_chip(chunk).wait_send()

    @pl.when(first_core)
    def _():
        for chunk in range(chunks):
            if chunk not in spread_chunks:
                for pair in range(1, ways // 2):
                    for origin in range(2):
                        passed(chunk, pair, origin).wait_send()

    @pl.when(jnp.logical_not(at_home))
    def _():
        answer(0).wait_send()


def deliver_kernel(*refs):
    sem = refs[-1]
    total = len(refs) // 2
    copies = [
        pltpu.make_async_copy(refs[index], refs[total + index], sem.at[index])
        for index in range(total)
    ]
    for copy in copies:
        copy.start()
    for copy in copies:
        copy.wait()


def one_step(
    tokens,
    norm_gain,
    weights,
    w_gates,
    forget_bias,
    head_gain,
    w_mix,
    state_cell,
    state_norm,
    state_max,
    pend_keys,
    pend_values,
    pend_gates,
    accepted,
):
    ways, groups = lax.axis_size("kv"), lax.axis_size("tp")
    seqs, proposals, model_width = tokens.shape
    count = seqs * proposals
    rows, width = weights[0].shape
    heads, head_size = state_norm.shape[1:]
    chunks = heads
    span = width // chunks
    f32, bf16 = jnp.float32, jnp.bfloat16

    def by_proposal(array):
        return array.transpose(1, 0, 2).reshape(count, array.shape[2])

    operands = (
        by_proposal(tokens),
        norm_gain[None, :],
        *weights,
        w_gates.transpose(1, 2, 0),
        forget_bias[None, :],
        head_gain[None, :],
        w_mix,
        state_cell,
        state_norm,
        state_max.T,
        by_proposal(pend_keys),
        by_proposal(pend_values),
        pend_gates.transpose(1, 2, 3, 0),
        accepted[None, :],
    )
    results = (
        ((count, ways // groups * width), bf16),
        (state_cell.shape, f32),
        (state_norm.shape, f32),
        ((heads, seqs), f32),
    )
    held = [jax.ShapeDtypeStruct(array.shape, array.dtype) for array in operands]
    held = held[:2] + [jax.ShapeDtypeStruct((chunks, rows, 4 * span), bf16)] + held[6:]
    held[6] = jax.ShapeDtypeStruct((2,) + w_mix.shape, bf16)
    block = (ways, count, rows)
    scratch = [pltpu.VMEM(array.shape, array.dtype) for array in held]
    scratch += [
        pltpu.VMEM(block, bf16),
        pltpu.VMEM(block, bf16),
        pltpu.VMEM((ways, 2, heads, rows), bf16),
        pltpu.VMEM((chunks, ways // 2, count, 4 * span), f32),
        pltpu.VMEM((chunks, ways, count, 4 * span), bf16),
        pltpu.VMEM((chunks, ways, count, 4 * span), bf16),
        pltpu.VMEM(((proposals + 2) * heads, 128), f32),
        pltpu.VMEM((heads, seqs * head_size, head_size), bf16),
        pltpu.VMEM((heads, seqs * head_size, head_size), bf16),
        pltpu.VMEM((heads, seqs, head_size), f32),
        pltpu.VMEM((proposals * (proposals + 5) // 2, seqs, 128), f32),
        pltpu.VMEM((count, head_size), f32),
        pltpu.VMEM((count, width), bf16),
        pltpu.VMEM((ways // 2, 2, count, width), bf16),
    ]
    scratch += [pltpu.VMEM((ways // 2, count, width), bf16)] * 2
    dma = pltpu.SemaphoreType.DMA
    scratch += [dma((len(operands) + 4 * chunks,))]
    scratch += [dma((ways,))] * 6
    scratch += [dma((chunks, ways))] * 5
    scratch += [dma(())] * 2
    scratch += [dma((ways,))] * 2
    hbm = pltpu.MemorySpace.HBM
    anywhere = pl.BlockSpec(memory_space=hbm)
    vmem = pl.BlockSpec(memory_space=pltpu.VMEM)
    held = pl.pallas_call(
        functools.partial(step_kernel, ways, groups, seqs),
        out_shape=tuple(pltpu.VMEM(shape, dtype) for shape, dtype in results),
        in_specs=[anywhere] * len(operands),
        out_specs=(vmem,) * len(results),
        scratch_shapes=scratch,
        compiler_params=pltpu.CompilerParams(
            collective_id=0, has_side_effects=True, vmem_limit_bytes=40 * 2**20
        ),
    )(*(pltpu.with_memory_space_constraint(array, hbm) for array in operands))
    mixed_out, cell_new, norm_new, max_new = pl.pallas_call(
        deliver_kernel,
        out_shape=tuple(jax.ShapeDtypeStruct(shape, dtype) for shape, dtype in results),
        in_specs=[vmem] * len(results),
        out_specs=(anywhere,) * len(results),
        scratch_shapes=[dma((len(results),))],
    )(*(pltpu.with_memory_space_constraint(array, pltpu.VMEM) for array in held))
    mixed_out = mixed_out.reshape(proposals, seqs, -1).transpose(1, 0, 2)
    return mixed_out, cell_new, norm_new, max_new.T


def project_by_digits(flat_rows, norm_gain, weights, w_mix):
    token_count, model_width = flat_rows.shape
    shard_rows = weights[0].shape[0]
    own = lax.axis_index("kv")
    kv_bits = lax.axis_size("kv").bit_length() - 1
    near_bits = kv_bits // 2
    near = 2**near_bits
    far = lax.axis_size("kv") // near
    digit_shape = (2,) * near_bits
    collected = collect_digits(
        weights + (w_mix,),
        (0, 0, 0, 0, 0, 1),
        own,
        range(near_bits, kv_bits),
        lambda parts, bit: jax.tree.map(
            lambda part, own: part.astype(own.dtype),
            from_partner(shortened(parts), "kv", bit),
            parts,
        ),
    )
    far_mix = collected[5]
    token_digits = jnp.moveaxis(flat_rows.reshape(token_count, far, near, shard_rows), 2, 0)
    token_digits = token_digits.reshape(digit_shape + (token_count, far, shard_rows))
    arrived = butterfly(
        token_digits, own, near_bits, lambda part, bit: from_partner(part, "kv", bit)
    )
    gathered = arrived.reshape(near * token_count, far * shard_rows)
    gain_part = lax.dynamic_index_in_dim(
        norm_gain.reshape(far, near, shard_rows), own % near, 1, keepdims=False
    ).reshape(far * shard_rows)
    widened = gathered.astype(jnp.float32)
    scaled_in = (widened * gain_part).astype(jnp.bfloat16)
    partials = tuple(
        (
            jnp.dot(scaled_in, weight, preferred_element_type=jnp.float32).reshape(
                digit_shape + (token_count, weight.shape[1])
            )
            for weight in collected[:5]
        )
    )
    part_squares = jnp.sum(widened * widened, axis=-1).reshape(digit_shape + (token_count,))
    summed = halving(
        partials + (part_squares,),
        own,
        near_bits,
        lambda parts, bit: jax.tree.map(
            lambda part, own: part.astype(own.dtype),
            from_partner(shortened(parts), "kv", bit),
            parts,
        ),
    )
    totals = summed[:5]
    sum_squares = summed[5]
    row_scale = lax.rsqrt(sum_squares / model_width + epsilon)[:, None]
    return (
        tuple((total * row_scale).astype(jnp.bfloat16) for total in totals[:4]),
        totals[4] * row_scale,
        far_mix,
    )


def mix_by_digits(gated_rows, far_mix, model_width):
    token_count = gated_rows.shape[0]
    shard_rows = model_width // lax.axis_size("kv")
    own = lax.axis_index("kv")
    kv_bits = lax.axis_size("kv").bit_length() - 1
    near_bits = kv_bits // 2
    near = 2**near_bits
    far = lax.axis_size("kv") // near
    digit_shape = (2,) * near_bits
    near_gated = collect_digits(
        (gated_rows,),
        (0,),
        own,
        range(near_bits),
        lambda parts, bit: jax.tree.map(
            lambda part, own: part.astype(own.dtype),
            from_partner(shortened(parts), "kv", bit),
            parts,
        ),
    )[0]
    group_part = jnp.dot(near_gated, far_mix, preferred_element_type=jnp.float32).astype(
        jnp.bfloat16
    )
    group_part = group_part.reshape(digit_shape + (token_count, far, shard_rows))
    placed = butterfly(group_part, own, near_bits, lambda part, bit: from_partner(part, "kv", bit))
    placed = placed.reshape(near, token_count, far, shard_rows).transpose(1, 2, 0, 3)
    partial_out = placed.reshape(token_count, model_width).astype(jnp.float32)
    mixed_out = lax.psum_scatter(
        partial_out.astype(jnp.bfloat16), "tp", scatter_dimension=1, tiled=True
    )
    return mixed_out


def shards(
    tokens,
    norm_gain,
    w_query,
    w_key,
    w_value,
    w_outgate,
    w_gates,
    forget_bias,
    head_gain,
    w_mix,
    state_cell,
    state_norm,
    state_max,
    pend_keys,
    pend_values,
    pend_gates,
    accepted,
):
    sequences, proposals, model_width = tokens.shape
    token_count = sequences * proposals
    local_heads = forget_bias.shape[0]
    head_size = state_cell.shape[-1]
    shard_rows = w_query.shape[0]
    weights = (w_query, w_key, w_value, w_outgate)
    ways, groups = lax.axis_size("kv"), lax.axis_size("tp")
    direct = (
        shard_rows % 256 == 0
        and w_mix.shape[1] == shard_rows
        and w_query.shape[1] == shard_rows
        and ways == 2 * groups
        and groups == 4
        and sequences == 8
        and head_size == 128
        and token_count <= head_size
    )
    if direct:
        return one_step(
            tokens,
            norm_gain,
            weights,
            w_gates,
            forget_bias,
            head_gain,
            w_mix,
            state_cell,
            state_norm,
            state_max,
            pend_keys,
            pend_values,
            pend_gates,
            accepted,
        )
    flat_gates = w_gates.reshape(shard_rows, -1)
    flat_rows = tokens.reshape(token_count, model_width)
    projected, gate_pre, far_mix = project_by_digits(
        flat_rows, norm_gain, weights + (flat_gates,), w_mix
    )
    queries, new_keys, new_values, outgate = projected
    gate_pre = gate_pre.reshape(sequences, proposals, 2, local_heads)

    def split_heads(array):
        return array.astype(jnp.float32).reshape(sequences, proposals, local_heads, head_size)

    key_scale = head_size ** (-0.5)
    cell_new, norm_new, new_max = fold_pending(
        state_cell,
        state_norm,
        state_max,
        split_heads(pend_keys) * key_scale,
        split_heads(pend_values),
        pend_gates,
        forget_bias,
        accepted,
    )
    log_in = gate_pre[:, :, 0, :]
    log_keep = jax.nn.log_sigmoid(gate_pre[:, :, 1, :] + forget_bias)
    hidden = read_block(
        split_heads(queries),
        split_heads(new_keys) * key_scale,
        split_heads(new_values),
        log_in,
        log_keep,
        cell_new,
        norm_new,
        new_max,
    )
    normed = hidden * lax.rsqrt(jnp.mean(hidden * hidden, axis=-1, keepdims=True) + epsilon)
    normed = normed * head_gain.reshape(local_heads, head_size)
    gated_rows = (jax.nn.sigmoid(split_heads(outgate)) * normed).astype(jnp.bfloat16)
    gated_rows = gated_rows.reshape(token_count, local_heads * head_size)
    mixed_out = mix_by_digits(gated_rows, far_mix, model_width)
    return (mixed_out.reshape(sequences, proposals, -1), cell_new, norm_new, new_max)


def solution(mesh):
    return jax.shard_map(
        shards,
        mesh=mesh,
        in_specs=(
            P("kv", None, None),
            P(),
            P("kv", "tp"),
            P("kv", "tp"),
            P("kv", "tp"),
            P("kv", "tp"),
            P("kv", None, "tp"),
            P("tp"),
            P("tp"),
            P("tp", "kv"),
            P("kv", "tp", None, None),
            P("kv", "tp", None),
            P("kv", "tp"),
            P("kv", None, "tp"),
            P("kv", None, "tp"),
            P("kv", None, None, "tp"),
            P("kv"),
        ),
        out_specs=(
            P("kv", None, "tp"),
            P("kv", "tp", None, None),
            P("kv", "tp", None),
            P("kv", "tp"),
        ),
        check_vma=False,
    )
```

```python
import functools

import jax
import jax.numpy as jnp
from jax import lax
from jax.experimental import pallas as pl
from jax.experimental.pallas import tpu as pltpu
from jax.sharding import PartitionSpec as P

epsilon = 1e-06
very_low = -1e30
highest = lax.Precision.HIGHEST


def shortened(shard):

    def short(part):
        return part.astype(jnp.bfloat16) if part.dtype == jnp.float32 else part

    return jax.tree.map(short, shard)


def from_partner(shard, axis, stride):
    return lax.ppermute(shard, axis, [(i, i ^ 1 << stride) for i in range(lax.axis_size(axis))])


def running_sum(values):
    steps = values.shape[1]
    upto = jnp.arange(steps)[:, None] >= jnp.arange(steps)[None, :]
    return jnp.sum(jnp.where(upto[None, :, :, None], values[:, None], 0.0), axis=2)


def fold_pending(
    cell_state, normer, stabilizer, key_rows, value_rows, gate_rows, forget_shift, accepted
):
    proposals = key_rows.shape[1]
    accepted_mask = jnp.arange(proposals)[None, :, None] < accepted[:, None, None]
    log_in = jnp.where(accepted_mask, gate_rows[:, :, 0, :], very_low)
    log_keep = jnp.where(
        accepted_mask, jax.nn.log_sigmoid(gate_rows[:, :, 1, :] + forget_shift), 0.0
    )
    running = running_sum(log_keep)
    block_total = running[:, -1]
    log_w = block_total[:, None, :] - running + log_in
    new_max = jnp.maximum(block_total + stabilizer, jnp.max(log_w, axis=1))
    weights = jnp.exp(log_w - new_max[:, None, :])
    carried = jnp.exp(block_total + stabilizer - new_max)
    weighted_keys = weights[..., None] * key_rows
    cell_new = carried[..., None, None] * cell_state + jnp.einsum(
        "sphd,sphe->shde", weighted_keys, value_rows, precision=highest
    )
    norm_new = carried[..., None] * normer + jnp.sum(weighted_keys, axis=1)
    return (cell_new, norm_new, new_max)


def read_block(queries, key_rows, value_rows, log_in, log_keep, cell_state, normer, stabilizer):
    proposals = queries.shape[1]
    causal = jnp.arange(proposals)[:, None] >= jnp.arange(proposals)[None, :]
    running_h = jnp.moveaxis(running_sum(log_keep), 1, 2)
    input_h = jnp.moveaxis(log_in, 1, 2)
    log_d = jnp.where(
        causal, running_h[..., :, None] - running_h[..., None, :] + input_h[..., None, :], very_low
    )
    log_p = running_h + stabilizer[..., None]
    top_log = jnp.maximum(log_p, jnp.max(log_d, axis=-1))
    decays = jnp.exp(log_d - top_log[..., None])
    prior_w = jnp.exp(log_p - top_log)
    scores = jnp.einsum("sthd,suhd->shtu", queries, key_rows, precision=highest) * decays
    numerator = jnp.einsum("shtu,suhe->shte", scores, value_rows, precision=highest)
    numerator = numerator + prior_w[..., None] * jnp.einsum(
        "sthd,shde->shte", queries, cell_state, precision=highest
    )
    denominator = jnp.sum(scores, axis=-1) + prior_w * jnp.einsum(
        "sthd,shd->sht", queries, normer, precision=highest
    )
    hidden_out = numerator / jnp.maximum(jnp.abs(denominator), jnp.exp(-top_log))[..., None]
    return jnp.moveaxis(hidden_out, 1, 2)


def digit_of(own, bit):
    return own // 2**bit % 2


def collect_digits(pieces, dims, own, bits, sender):
    for bit in bits:
        others = sender(pieces, bit)
        first = digit_of(own, bit) == 0
        pieces = tuple(
            (
                jnp.where(
                    first,
                    jnp.concatenate((mine, theirs), axis=dim),
                    jnp.concatenate((theirs, mine), axis=dim),
                )
                for mine, theirs, dim in zip(pieces, others, dims)
            )
        )
    return pieces


def butterfly(blocks, own, near_bits, sender):
    for bit in range(near_bits):
        axis = near_bits - 1 - bit
        mine_digit = digit_of(own, bit)
        kept = lax.dynamic_index_in_dim(blocks, mine_digit, axis, keepdims=False)
        outgoing = lax.dynamic_index_in_dim(blocks, 1 - mine_digit, axis, keepdims=False)
        arrived = sender(outgoing, bit)
        blocks = jnp.where(
            mine_digit == 0,
            jnp.stack((kept, arrived), axis=axis),
            jnp.stack((arrived, kept), axis=axis),
        )
    return blocks


def halving(terms, own, near_bits, sender):
    for bit in range(near_bits - 1, -1, -1):
        mine_digit = digit_of(own, bit)
        kept = tuple(
            (lax.dynamic_index_in_dim(term, mine_digit, 0, keepdims=False) for term in terms)
        )
        outgoing = tuple(
            (lax.dynamic_index_in_dim(term, 1 - mine_digit, 0, keepdims=False) for term in terms)
        )
        arrived = sender(outgoing, bit)
        terms = tuple((left + right for left, right in zip(kept, arrived)))
    return terms


def log_sigmoid(values):
    return jnp.minimum(values, 0.0) - jnp.log1p(jnp.exp(-jnp.abs(values)))


def flipped(index, bits):
    place = 1
    while place <= bits:
        if bits // place % 2:
            index = index + place * (1 - 2 * (index // place % 2))
        place *= 2
    return index


spread_chunks = (2, 3)
tasks = (
    ("forward", 7),
    ("forward", 3),
    ("gate fold", 0),
    ("forward", 6),
    ("forward", 5),
    ("forward", 4),
    ("weights", 0),
    ("arrive", 7),
    ("multiply", 7),
    ("send", (7, 0)),
    ("send", (7, 1)),
    ("arrive", 3),
    ("multiply", 3),
    ("send", (3, 0)),
    ("send", (3, 1)),
    ("arrive", 6),
    ("multiply", 6),
    ("send", (6, 0)),
    ("send", (6, 1)),
    ("arrive", 5),
    ("multiply", 5),
    ("send", (5, 0)),
    ("send", (5, 1)),
    ("send", (7, 2)),
    ("send", (3, 2)),
    ("send", (5, 2)),
    ("send", (7, 3)),
    ("send", (3, 3)),
    ("send", (5, 3)),
    ("arrive", 4),
    ("multiply", 4),
    ("multiply", 0),
    ("fold", 0),
    ("fold", 1),
    ("fold", 2),
    ("fold", 3),
    (0, 0),
    (0, 1),
    (1, 0),
    ("squares", 0),
    ("gates", 0),
    (0, 2),
    (1, 1),
    (0, 3),
    (1, 2),
    (2, 1),
    (2, 0),
    (1, 3),
    (2, 2),
    ("pass", 1),
    ("pass", 0),
    ("mix", 0),
    ("mix", 1),
)


def step_kernel(
    ways,
    groups,
    seqs,
    tok_hbm,
    gain_hbm,
    wq_hbm,
    wk_hbm,
    wv_hbm,
    wo_hbm,
    wg_hbm,
    bias_hbm,
    head_gain_hbm,
    mix_hbm,
    cell_hbm,
    norm_hbm,
    max_hbm,
    pend_k_hbm,
    pend_v_hbm,
    pend_g_hbm,
    accepted_hbm,
    out,
    cell_new,
    norm_new,
    max_new,
    tok,
    gain,
    weights,
    wg,
    bias,
    head_gain,
    mix_w,
    cell,
    norm,
    stab,
    pend_k,
    pend_v,
    pend_g,
    accepted,
    tok_in,
    scaled,
    wg_in,
    sums,
    part_out,
    part_in,
    fold_rows,
    cell_high,
    cell_low,
    norm_head,
    decay,
    scale_col,
    keys,
    values,
    gated,
    gated_in,
    answer_out,
    answer_in,
    load_sem,
    tok_send,
    tok_recv,
    fwd_send,
    fwd_recv,
    wg_send,
    wg_recv,
    part_send,
    part_recv,
    gated_send,
    gated_recv,
    pass_send,
    mix_send,
    mix_recv,
    answer_send,
    answer_recv,
):
    me = lax.axis_index("kv")
    group = lax.axis_index("tp")
    across, core = group // 2, lax.rem(group, 2)
    side = lax.rem(me, 2)
    count, model_width = tok.shape
    rows = model_width // ways
    half = rows // 2
    chunks, span = weights.shape[0], weights.shape[2] // 4
    heads, head_size = norm.shape[1], norm.shape[2]
    proposals = count // seqs
    cut = count // 2
    pair_heads = heads // 2
    bits = ways.bit_length() - 1
    f32, bf16 = jnp.float32, jnp.bfloat16
    near_first = tuple(range(bits))
    far_first = near_first[1:] + near_first[:1]
    plans = [(near_first, False)] * chunks
    plans[0] = (far_first, False)
    plans[-1] = (near_first, True)

    def first_bit(chunk):
        return 1 << plans[chunk][0][0]

    def slot(chunk, shift):
        return sum(1 for other in range(shift) if not other & first_bit(chunk))


    loads = {}

    def load(name, source, target):
        copy = pltpu.make_async_copy(source, target, load_sem.at[len(loads)])
        copy.start()
        loads[name] = copy

    load("tok", tok_hbm, tok)
    load("gain", gain_hbm, gain)
    for chunk in range(chunks):
        for index, source in enumerate((wq_hbm, wk_hbm, wv_hbm, wo_hbm)):
            load(
                ("weight", chunk, index),
                source.at[:, chunk * span : (chunk + 1) * span],
                weights.at[chunk, :, index * span : (index + 1) * span],
            )
    load("wg", wg_hbm, wg)
    load("bias", bias_hbm, bias)
    load("max", max_hbm, stab)
    load("pend_g", pend_g_hbm, pend_g)
    load("accepted", accepted_hbm, accepted)
    load("pend_k", pend_k_hbm, pend_k)
    load("pend_v", pend_v_hbm, pend_v)
    load("norm", norm_hbm, norm)
    load("cell", cell_hbm, cell)
    load("head_gain", head_gain_hbm, head_gain)
    load("mix", mix_hbm, mix_w.at[core])

    target = me // 2
    at_home = jnp.logical_and(target == group, core == 0)
    barrier = pltpu.get_barrier_semaphore()

    def signal(where):
        pl.semaphore_signal(
            barrier, inc=1, device_id=where, device_id_type=pl.DeviceIdType.MESH
        )

    partner = {"tp": 2 * across + 1 - core}
    for shift in range(1, ways):
        for other in range(2):
            signal({"kv": flipped(me, shift), "tp": 2 * across + other})
    signal(partner)
    for which in range(2):
        sender = 2 * group + which
        sender_core = side + which - 2 * side * which
        for other in range(groups // 2):
            sender_group = 2 * other + sender_core

            @pl.when(jnp.logical_or(sender != me, sender_group != group))
            def _():
                signal({"kv": sender, "tp": sender_group})

    greetings = 2 * (ways - 1) + 1 + ways // 2

    @pl.when(at_home)
    def _():
        pl.semaphore_wait(barrier, greetings - 1)

    @pl.when(jnp.logical_not(at_home))
    def _():
        pl.semaphore_wait(barrier, greetings)

    sends = []

    def remote(source, target_ref, send_sem, recv_sem, where):
        copy = pltpu.make_async_remote_copy(
            src_ref=source,
            dst_ref=target_ref,
            send_sem=send_sem,
            recv_sem=recv_sem,
            device_id=where,
            device_id_type=pl.DeviceIdType.MESH,
        )
        copy.start()
        sends.append(copy)
        return copy

    def columns(owner):
        return pl.ds(pl.multiple_of(owner * rows, rows), rows)

    halves = pl.ds(pl.multiple_of(core * half, half), half)

    tok_copies, fwd_copies, wg_copies = {}, {}, {}
    loads["tok"].wait()
    whole = (1, 2)

    def send_tokens(shift):
        there = flipped(me, shift)
        if shift in whole:
            source, place = tok.at[:, columns(there)], tok_in.at[shift]
        else:
            source = tok.at[:, pl.ds(pl.multiple_of(there * rows + core * half, half), half)]
            place = tok_in.at[shift, :, halves]
        tok_copies[shift] = remote(
            source, place, tok_send.at[shift], tok_recv.at[shift], {"kv": there}
        )

    others = [shift for shift in (7, 3, 6, 5, 4) if shift < ways]
    for shift in list(whole) + others:
        send_tokens(shift)

    loads["gain"].wait()
    own_gain = gain[:, columns(me)]

    def scale_block(shift, block):
        scaled[shift] = (block.astype(f32) * own_gain).astype(bf16)

    def forward(shift):
        tok_copies[shift].wait_recv()
        place = tok_in.at[shift, :, halves]
        fwd_copies[shift] = remote(
            place, place, fwd_send.at[shift], fwd_recv.at[shift], partner
        )

    def arrive(shift):
        if shift in whole:
            tok_copies[shift].wait_recv()
        else:
            fwd_copies[shift].wait_recv()
        scale_block(shift, tok_in[shift])

    def half_rows(array, part):
        return array[part * cut : (part + 1) * cut]

    part_copies = {}
    mix_copy = []

    def start_part(chunk, shift, move):
        part_copies[chunk, shift] = remote(
            part_out.at[chunk, shift],
            part_in.at[chunk, shift],
            part_send.at[chunk, shift],
            part_recv.at[chunk, shift],
            {"kv": flipped(me, move)},
        )

    def send_part(chunk, shift, move, value):
        part_out[chunk, shift] = value.astype(bf16)
        start_part(chunk, shift, move)

    def first_send(chunk, shift):
        if shift & first_bit(chunk):
            start_part(chunk, shift, first_bit(chunk))

    def multiply(shift):
        for pair in range(2):
            products = [
                jnp.dot(scaled[shift], weights[head], preferred_element_type=f32)
                for head in range(pair * pair_heads, (pair + 1) * pair_heads)
            ]
            for part in range(2):
                chunk = 2 * part + pair
                value = jnp.concatenate([half_rows(each, part) for each in products], axis=0)
                if shift & first_bit(chunk):
                    part_out[chunk, shift] = value.astype(bf16)
                else:
                    sums[chunk, slot(chunk, shift)] = value

    scale_block(0, tok[:, columns(me)])
    for chunk in range(chunks):
        for index in range(4):
            loads["weight", chunk, index].wait()

    for shift in whole:
        arrive(shift)
        multiply(shift)
        for chunk in range(chunks):
            first_send(chunk, shift)

    def send_gates():
        loads["mix"].wait()
        mix_copy.append(remote(mix_w.at[core], mix_w.at[core], mix_send, mix_recv, partner))
        loads["wg"].wait()
        for shift in range(1, ways):
            wg_copies[shift] = remote(
                wg,
                wg_in.at[shift],
                wg_send.at[shift],
                wg_recv.at[shift],
                {"kv": flipped(me, shift)},
            )

    def square_rows():
        squares = jnp.zeros((count, 1), f32)
        for step in range(ways):
            part = tok[:, step * rows : (step + 1) * rows].astype(f32)
            squares = squares + jnp.sum(part * part, axis=1, keepdims=True)
        row_scale = lax.rsqrt(squares / model_width + epsilon)
        scale_col[...] = jnp.broadcast_to(row_scale, scale_col.shape)

    def eye(size):
        across_rows = lax.broadcasted_iota(jnp.int32, (size, size), 0)
        return across_rows == lax.broadcasted_iota(jnp.int32, (size, size), 1)

    def fold_gates():
        for name in ("bias", "max", "pend_g", "accepted"):
            loads[name].wait()
        bias_col = jnp.sum(
            jnp.where(eye(heads), jnp.broadcast_to(bias[...], (heads, heads)), 0.0),
            axis=1,
            keepdims=True,
        )
        log_in, running = [], []
        total = jnp.zeros((heads, seqs), f32)
        for step in range(proposals):
            taken = jnp.broadcast_to(step < accepted[...], (heads, seqs))
            log_in.append(jnp.where(taken, pend_g[step, 0], very_low))
            total = total + jnp.where(taken, log_sigmoid(pend_g[step, 1] + bias_col), 0.0)
            running.append(total)
        log_w = [total - at + ins for at, ins in zip(running, log_in)]
        carried_log = total + stab[...]
        top = carried_log
        for values in log_w:
            top = jnp.maximum(top, values)
        max_new[...] = top
        fold_rows[...] = jnp.zeros(fold_rows.shape, f32)
        pieces = [jnp.exp(values - top) for values in log_w]
        pieces = pieces + [jnp.exp(carried_log - top), top]
        for index, piece in enumerate(pieces):
            fold_rows[index * heads : (index + 1) * heads, 0:seqs] = piece
        return fold_rows[...].T[:seqs]

    key_scale = head_size ** (-0.5)

    def fold_head(cols, head):
        lanes = slice(head * head_size, (head + 1) * head_size)
        keys = pend_k[:, lanes].astype(f32)
        weighted = []
        carried = jnp.broadcast_to(
            cols[:, proposals * heads + head : proposals * heads + head + 1], (seqs, head_size)
        )
        key_sum = carried * norm[:, head, :]
        for step in range(proposals):
            weight = cols[:, step * heads + head : step * heads + head + 1]
            rows_at = keys[step * seqs : (step + 1) * seqs] * key_scale * weight
            weighted.append(rows_at)
            key_sum = key_sum + rows_at
        norm_head[head] = key_sum
        norm_new[:, head, :] = key_sum
        padding = jnp.zeros((head_size - count, head_size), f32)
        turned = jnp.concatenate(weighted + [padding], axis=0).T
        value_rows = jnp.concatenate(
            [pend_v[:, lanes].astype(f32), padding], axis=0
        ).astype(bf16)
        value_rows = jnp.concatenate([value_rows, value_rows], axis=0)
        high = turned.astype(bf16).astype(f32)
        low = turned - high
        lane = lax.rem(lax.broadcasted_iota(jnp.int32, turned.shape, 1), seqs)
        for seq in range(seqs):
            mine = lane == seq
            left = jnp.concatenate(
                [jnp.where(mine, high, 0.0).astype(bf16), jnp.where(mine, low, 0.0).astype(bf16)],
                axis=1,
            )
            update = jnp.dot(left, value_rows, preferred_element_type=f32)
            result = carried[seq : seq + 1] * cell[seq, head] + update
            cell_new[seq, head] = result
            upper = result.astype(bf16)
            at = slice(seq * head_size, (seq + 1) * head_size)
            cell_high[head, at, :] = upper
            cell_low[head, at, :] = (result - upper.astype(f32)).astype(bf16)

    cols = []

    contract = (((1,), (1,)), ((), ()))

    def read_gates():
        gates = [jnp.zeros((count, heads), f32)] * 2
        for shift in range(ways):
            owner = flipped(me, shift)
            if shift:
                wg_copies[shift].wait_recv()
                block = (tok[:, columns(owner)].astype(f32) * gain[:, columns(owner)]).astype(bf16)
            else:
                block = scaled[0]
            for part in range(2):
                right = wg_in[shift, part] if shift else wg[part]
                gates[part] = gates[part] + lax.dot_general(
                    block, right, contract, preferred_element_type=f32
                )
        stabilizer = cols[0][:, (proposals + 1) * heads : (proposals + 2) * heads]
        log_in, running = [], []
        total = jnp.zeros((seqs, heads), f32)
        scale = scale_col[:, :1]
        gate_in, gate_keep = gates[0] * scale, gates[1] * scale
        index = 0
        for step in range(proposals):
            at = slice(step * seqs, (step + 1) * seqs)
            log_in.append(gate_in[at])
            total = total + log_sigmoid(gate_keep[at] + bias[...])
            running.append(total)
            log_p = total + stabilizer
            log_d = [total - running[past] + log_in[past] for past in range(step + 1)]
            top = log_p
            for values in log_d:
                top = jnp.maximum(top, values)
            for values in log_d + [log_p, None]:
                decay[index, :, :heads] = jnp.exp(-top if values is None else values - top)
                index += 1

    first_core, second_core = core == 0, core == 1

    def gated_copy(chunk, source, pair, origin, send_sem, there, there_core):
        return pltpu.make_async_remote_copy(
            src_ref=source,
            dst_ref=gated_in.at[pair, origin, chunk],
            send_sem=send_sem,
            recv_sem=gated_recv.at[chunk, 2 * pair + origin],
            device_id={"kv": there, "tp": 2 * across + there_core},
            device_id_type=pl.DeviceIdType.MESH,
        )

    def to_own_chip(chunk):
        return gated_copy(chunk, gated.at[chunk], 0, core, gated_send.at[chunk, 0], me, 0)

    def arrived(chunk, pair, origin):
        pltpu.make_async_copy(
            gated.at[chunk],
            gated_in.at[pair, origin, chunk],
            gated_recv.at[chunk, 2 * pair + origin],
        ).wait()

    def passed(chunk, pair, origin):
        return gated_copy(
            chunk,
            gated_in.at[pair, origin, chunk],
            pair,
            origin,
            pass_send.at[chunk, 2 * pair + origin],
            flipped(me, 1),
            1,
        )

    def send_gated(chunk):
        for shift in range(ways - 1, 0, -1):
            if chunk in spread_chunks or shift == 1 or not shift % 2:
                copy = gated_copy(
                    chunk,
                    gated.at[chunk],
                    shift // 2,
                    core,
                    gated_send.at[chunk, shift],
                    flipped(me, shift),
                    shift % 2,
                )
                copy.start()
                sends.append(copy)

        @pl.when(second_core)
        def _():
            to_own_chip(chunk).start()

        @pl.when(first_core)
        def _():
            pltpu.make_async_copy(
                gated.at[chunk], gated_in.at[0, 0, chunk], gated_recv.at[chunk, 0]
            ).start()

    def pass_gated(chunk):
        @pl.when(first_core)
        def _():
            for pair in range(ways // 2 - 1, 0, -1):
                for origin in range(2):
                    arrived(chunk, pair, origin)
                    passed(chunk, pair, origin).start()

    def read_head(head, part, flat):
        scale = scale_col[part * cut : (part + 1) * cut]
        half_steps = proposals // 2

        def piece(index):
            at = index * head_size
            return (flat[:, at : at + head_size] * scale).astype(bf16).astype(f32)

        query, key, value, outgate = (piece(index) for index in range(4))
        keys[head, part * cut : (part + 1) * cut] = key * key_scale
        values[head, part * cut : (part + 1) * cut] = value
        sequence = lax.rem(lax.broadcasted_iota(jnp.int32, query.shape, 0), seqs)
        spread = jnp.concatenate(
            [jnp.where(sequence == seq, query, 0.0).astype(bf16) for seq in range(seqs)], axis=1
        )
        prior = jnp.dot(spread, cell_high[head], preferred_element_type=f32)
        prior = prior + jnp.dot(spread, cell_low[head], preferred_element_type=f32)
        normer = norm_head[head]
        hidden = []
        for step in range(part * half_steps, (part + 1) * half_steps):
            index = step * (step + 5) // 2
            at = slice((step - part * half_steps) * seqs, (step - part * half_steps + 1) * seqs)
            now = query[at]
            numerator, denominator = None, None

            def factor(which):
                return decay[which, :, head : head + 1]

            for past in range(step + 1):
                before = slice(past * seqs, (past + 1) * seqs)
                score = jnp.sum(now * keys[head, before], axis=1, keepdims=True)
                score = score * factor(index + past)
                term = score * values[head, before]
                numerator = term if numerator is None else numerator + term
                denominator = score if denominator is None else denominator + score
            prior_w = factor(index + step + 1)
            numerator = numerator + prior_w * prior[at]
            denominator = denominator + prior_w * jnp.sum(now * normer, axis=1, keepdims=True)
            floor = factor(index + step + 2)
            hidden.append(numerator / jnp.maximum(jnp.abs(denominator), floor))
        hidden = jnp.concatenate(hidden, axis=0)
        normed = hidden * lax.rsqrt(jnp.mean(hidden * hidden, axis=1, keepdims=True) + epsilon)
        normed = normed * head_gain[:, head * head_size : (head + 1) * head_size]
        return jax.nn.sigmoid(outgate) * normed

    def complete(chunk, value):
        part, pair = chunk // 2, chunk % 2
        done = [
            read_head(pair * pair_heads + local, part, half_rows(value, local))
            for local in range(pair_heads)
        ]
        gated[chunk] = jnp.concatenate(done, axis=0).astype(bf16)
        send_gated(chunk)

    def take(chunk, stage):
        order, straight = plans[chunk]
        if straight and stage:
            value = sums[chunk, 0]
            for shift in range(1, ways):
                if not shift & first_bit(chunk):
                    part_copies[chunk, shift].wait_recv()
                    value = value + part_in[chunk, shift].astype(f32)
            complete(chunk, value)
            return
        bit = 1 << order[stage]
        done = sum(1 << b for b in order[: stage + 1])
        later = [1 << b for b in order[stage + 1 :]]
        places = [shift for shift in range(ways) if not shift & done]
        places.sort(key=lambda shift: tuple(-(shift // b % 2) for b in later))
        for shift in places:
            part_copies[chunk, shift + bit].wait_recv()
            value = sums[chunk, slot(chunk, shift)] + part_in[chunk, shift + bit].astype(f32)
            if straight and shift:
                send_part(chunk, shift, shift, value)
            elif later and shift & later[0]:
                send_part(chunk, shift, later[0], value)
            elif later:
                sums[chunk, slot(chunk, shift)] = value
            else:
                complete(chunk, value)

    spot = side * (groups // 2) + across

    def answer(part, pair):
        owner = flipped(me, 2 * pair) + core * (1 - 2 * side)
        return pltpu.make_async_remote_copy(
            src_ref=answer_out.at[part, pair],
            dst_ref=answer_in.at[part, spot],
            send_sem=answer_send.at[part, pair],
            recv_sem=answer_recv.at[part, spot],
            device_id={"kv": owner, "tp": target},
            device_id_type=pl.DeviceIdType.MESH,
        )

    def at_own(part):
        return pltpu.make_async_copy(
            answer_out.at[part, 0], answer_in.at[part, spot], answer_recv.at[part, spot]
        )

    width = mix_w.shape[2]
    wide = width // 2

    def mix_half(part):
        ours = (2 * part, 2 * part + 1)
        for pair in range(ways // 2):
            for chunk in ours:
                if chunk in spread_chunks or not pair:
                    for origin in range(2):
                        arrived(chunk, pair, origin)
                else:

                    @pl.when(second_core)
                    def _():
                        for origin in range(2):
                            arrived(chunk, pair, origin)

            value = jnp.zeros((cut, width), f32)
            for origin in range(2):
                blocks = [gated_in[pair, origin, chunk].astype(f32) for chunk in ours]
                left = jnp.concatenate(
                    [half_rows(block, local) for block in blocks for local in range(2)], axis=1
                ).astype(bf16)
                value = value + jnp.dot(left, mix_w[origin], preferred_element_type=f32)
            stacked = jnp.concatenate([value[:, :wide], value[:, wide:]], axis=0)
            answer_out[part, pair] = stacked.astype(bf16)
            if pair:
                copy = answer(part, pair)
                copy.start()
                sends.append(copy)
            else:

                @pl.when(at_home)
                def _():
                    at_own(part).start()

                @pl.when(jnp.logical_not(at_home))
                def _():
                    answer(part, 0).start()

    for kind, which in tasks:
        if kind == "forward":
            forward(which)
        elif kind == "arrive":
            arrive(which)
        elif kind == "send":
            first_send(which[1], which[0])
        elif kind == "multiply":
            multiply(which)
        elif kind == "mix":
            if not which:
                mix_copy[0].wait_recv()
            mix_half(which)
        elif kind == "gate fold":
            cols.append(fold_gates())
        elif kind == "fold":
            if not which:
                for name in ("pend_k", "pend_v", "norm", "cell"):
                    loads[name].wait()
            fold_head(cols[0], which)
        elif kind == "weights":
            send_gates()
        elif kind == "squares":
            square_rows()
        elif kind == "gates":
            loads["head_gain"].wait()
            read_gates()
        elif kind == "pass":
            pass_gated(which)
        else:
            take(which, kind)

    for which in range(2):
        totals = []
        for part in range(2):
            total = None
            for other in range(groups // 2):
                spot_at = which * (groups // 2) + other
                pltpu.make_async_copy(
                    answer_out.at[part, 0],
                    answer_in.at[part, spot_at],
                    answer_recv.at[part, spot_at],
                ).wait()
                term = answer_in[part, spot_at].astype(f32)
                total = term if total is None else total + term
            totals.append(total)
        for side_cols in range(2):
            both = jnp.concatenate([half_rows(total, side_cols) for total in totals], axis=0)
            at = which * width + side_cols * wide
            out[:, at : at + wide] = both.astype(bf16)
    for copy in sends:
        copy.wait_send()

    @pl.when(second_core)
    def _():
        for chunk in range(chunks):
            to_own_chip(chunk).wait_send()

    @pl.when(first_core)
    def _():
        for chunk in range(chunks):
            if chunk not in spread_chunks:
                for pair in range(1, ways // 2):
                    for origin in range(2):
                        passed(chunk, pair, origin).wait_send()

    @pl.when(jnp.logical_not(at_home))
    def _():
        for part in range(2):
            answer(part, 0).wait_send()


def deliver_kernel(*refs):
    sem = refs[-1]
    total = len(refs) // 2
    copies = [
        pltpu.make_async_copy(refs[index], refs[total + index], sem.at[index])
        for index in range(total)
    ]
    for copy in copies:
        copy.start()
    for copy in copies:
        copy.wait()


def one_step(
    tokens,
    norm_gain,
    weights,
    w_gates,
    forget_bias,
    head_gain,
    w_mix,
    state_cell,
    state_norm,
    state_max,
    pend_keys,
    pend_values,
    pend_gates,
    accepted,
):
    ways, groups = lax.axis_size("kv"), lax.axis_size("tp")
    seqs, proposals, model_width = tokens.shape
    count = seqs * proposals
    rows, width = weights[0].shape
    heads, head_size = state_norm.shape[1:]
    chunks = heads
    span = width // chunks
    f32, bf16 = jnp.float32, jnp.bfloat16

    def by_proposal(array):
        return array.transpose(1, 0, 2).reshape(count, array.shape[2])

    operands = (
        by_proposal(tokens),
        norm_gain[None, :],
        *weights,
        w_gates.transpose(1, 2, 0),
        forget_bias[None, :],
        head_gain[None, :],
        w_mix,
        state_cell,
        state_norm,
        state_max.T,
        by_proposal(pend_keys),
        by_proposal(pend_values),
        pend_gates.transpose(1, 2, 3, 0),
        accepted[None, :],
    )
    results = (
        ((count, ways // groups * width), bf16),
        (state_cell.shape, f32),
        (state_norm.shape, f32),
        ((heads, seqs), f32),
    )
    held = [jax.ShapeDtypeStruct(array.shape, array.dtype) for array in operands]
    held = held[:2] + [jax.ShapeDtypeStruct((chunks, rows, 4 * span), bf16)] + held[6:]
    held[6] = jax.ShapeDtypeStruct((2,) + w_mix.shape, bf16)
    block = (ways, count, rows)
    scratch = [pltpu.VMEM(array.shape, array.dtype) for array in held]
    scratch += [
        pltpu.VMEM(block, bf16),
        pltpu.VMEM(block, bf16),
        pltpu.VMEM((ways, 2, heads, rows), bf16),
        pltpu.VMEM((chunks, ways // 2, count, 4 * span), f32),
        pltpu.VMEM((chunks, ways, count, 4 * span), bf16),
        pltpu.VMEM((chunks, ways, count, 4 * span), bf16),
        pltpu.VMEM(((proposals + 2) * heads, 128), f32),
        pltpu.VMEM((heads, seqs * head_size, head_size), bf16),
        pltpu.VMEM((heads, seqs * head_size, head_size), bf16),
        pltpu.VMEM((heads, seqs, head_size), f32),
        pltpu.VMEM((proposals * (proposals + 5) // 2, seqs, 128), f32),
        pltpu.VMEM((count, head_size), f32),
        pltpu.VMEM((heads, count, head_size), f32),
        pltpu.VMEM((heads, count, head_size), f32),
        pltpu.VMEM((chunks, count, span), bf16),
        pltpu.VMEM((ways // 2, 2, chunks, count, span), bf16),
    ]
    scratch += [pltpu.VMEM((2, ways // 2, count, width // 2), bf16)] * 2
    dma = pltpu.SemaphoreType.DMA
    scratch += [dma((len(operands) + 4 * chunks,))]
    scratch += [dma((ways,))] * 6
    scratch += [dma((chunks, ways))] * 5
    scratch += [dma(())] * 2
    scratch += [dma((2, ways // 2))] * 2
    hbm = pltpu.MemorySpace.HBM
    anywhere = pl.BlockSpec(memory_space=hbm)
    vmem = pl.BlockSpec(memory_space=pltpu.VMEM)
    held = pl.pallas_call(
        functools.partial(step_kernel, ways, groups, seqs),
        out_shape=tuple(pltpu.VMEM(shape, dtype) for shape, dtype in results),
        in_specs=[anywhere] * len(operands),
        out_specs=(vmem,) * len(results),
        scratch_shapes=scratch,
        compiler_params=pltpu.CompilerParams(
            collective_id=0, has_side_effects=True, vmem_limit_bytes=40 * 2**20
        ),
    )(*(pltpu.with_memory_space_constraint(array, hbm) for array in operands))
    mixed_out, cell_new, norm_new, max_new = pl.pallas_call(
        deliver_kernel,
        out_shape=tuple(jax.ShapeDtypeStruct(shape, dtype) for shape, dtype in results),
        in_specs=[vmem] * len(results),
        out_specs=(anywhere,) * len(results),
        scratch_shapes=[dma((len(results),))],
    )(*(pltpu.with_memory_space_constraint(array, pltpu.VMEM) for array in held))
    mixed_out = mixed_out.reshape(proposals, seqs, -1).transpose(1, 0, 2)
    return mixed_out, cell_new, norm_new, max_new.T


def project_by_digits(flat_rows, norm_gain, weights, w_mix):
    token_count, model_width = flat_rows.shape
    shard_rows = weights[0].shape[0]
    own = lax.axis_index("kv")
    kv_bits = lax.axis_size("kv").bit_length() - 1
    near_bits = kv_bits // 2
    near = 2**near_bits
    far = lax.axis_size("kv") // near
    digit_shape = (2,) * near_bits
    collected = collect_digits(
        weights + (w_mix,),
        (0, 0, 0, 0, 0, 1),
        own,
        range(near_bits, kv_bits),
        lambda parts, bit: jax.tree.map(
            lambda part, own: part.astype(own.dtype),
            from_partner(shortened(parts), "kv", bit),
            parts,
        ),
    )
    far_mix = collected[5]
    token_digits = jnp.moveaxis(flat_rows.reshape(token_count, far, near, shard_rows), 2, 0)
    token_digits = token_digits.reshape(digit_shape + (token_count, far, shard_rows))
    arrived = butterfly(
        token_digits, own, near_bits, lambda part, bit: from_partner(part, "kv", bit)
    )
    gathered = arrived.reshape(near * token_count, far * shard_rows)
    gain_part = lax.dynamic_index_in_dim(
        norm_gain.reshape(far, near, shard_rows), own % near, 1, keepdims=False
    ).reshape(far * shard_rows)
    widened = gathered.astype(jnp.float32)
    scaled_in = (widened * gain_part).astype(jnp.bfloat16)
    partials = tuple(
        (
            jnp.dot(scaled_in, weight, preferred_element_type=jnp.float32).reshape(
                digit_shape + (token_count, weight.shape[1])
            )
            for weight in collected[:5]
        )
    )
    part_squares = jnp.sum(widened * widened, axis=-1).reshape(digit_shape + (token_count,))
    summed = halving(
        partials + (part_squares,),
        own,
        near_bits,
        lambda parts, bit: jax.tree.map(
            lambda part, own: part.astype(own.dtype),
            from_partner(shortened(parts), "kv", bit),
            parts,
        ),
    )
    totals = summed[:5]
    sum_squares = summed[5]
    row_scale = lax.rsqrt(sum_squares / model_width + epsilon)[:, None]
    return (
        tuple((total * row_scale).astype(jnp.bfloat16) for total in totals[:4]),
        totals[4] * row_scale,
        far_mix,
    )


def mix_by_digits(gated_rows, far_mix, model_width):
    token_count = gated_rows.shape[0]
    shard_rows = model_width // lax.axis_size("kv")
    own = lax.axis_index("kv")
    kv_bits = lax.axis_size("kv").bit_length() - 1
    near_bits = kv_bits // 2
    near = 2**near_bits
    far = lax.axis_size("kv") // near
    digit_shape = (2,) * near_bits
    near_gated = collect_digits(
        (gated_rows,),
        (0,),
        own,
        range(near_bits),
        lambda parts, bit: jax.tree.map(
            lambda part, own: part.astype(own.dtype),
            from_partner(shortened(parts), "kv", bit),
            parts,
        ),
    )[0]
    group_part = jnp.dot(near_gated, far_mix, preferred_element_type=jnp.float32).astype(
        jnp.bfloat16
    )
    group_part = group_part.reshape(digit_shape + (token_count, far, shard_rows))
    placed = butterfly(group_part, own, near_bits, lambda part, bit: from_partner(part, "kv", bit))
    placed = placed.reshape(near, token_count, far, shard_rows).transpose(1, 2, 0, 3)
    partial_out = placed.reshape(token_count, model_width).astype(jnp.float32)
    mixed_out = lax.psum_scatter(
        partial_out.astype(jnp.bfloat16), "tp", scatter_dimension=1, tiled=True
    )
    return mixed_out


def shards(
    tokens,
    norm_gain,
    w_query,
    w_key,
    w_value,
    w_outgate,
    w_gates,
    forget_bias,
    head_gain,
    w_mix,
    state_cell,
    state_norm,
    state_max,
    pend_keys,
    pend_values,
    pend_gates,
    accepted,
):
    sequences, proposals, model_width = tokens.shape
    token_count = sequences * proposals
    local_heads = forget_bias.shape[0]
    head_size = state_cell.shape[-1]
    shard_rows = w_query.shape[0]
    weights = (w_query, w_key, w_value, w_outgate)
    ways, groups = lax.axis_size("kv"), lax.axis_size("tp")
    direct = (
        shard_rows % 256 == 0
        and w_mix.shape[1] == shard_rows
        and w_query.shape[1] == shard_rows
        and ways == 2 * groups
        and groups == 4
        and local_heads == 4
        and proposals % 2 == 0
        and sequences == 8
        and head_size == 128
        and token_count <= head_size
    )
    if direct:
        return one_step(
            tokens,
            norm_gain,
            weights,
            w_gates,
            forget_bias,
            head_gain,
            w_mix,
            state_cell,
            state_norm,
            state_max,
            pend_keys,
            pend_values,
            pend_gates,
            accepted,
        )
    flat_gates = w_gates.reshape(shard_rows, -1)
    flat_rows = tokens.reshape(token_count, model_width)
    projected, gate_pre, far_mix = project_by_digits(
        flat_rows, norm_gain, weights + (flat_gates,), w_mix
    )
    queries, new_keys, new_values, outgate = projected
    gate_pre = gate_pre.reshape(sequences, proposals, 2, local_heads)

    def split_heads(array):
        return array.astype(jnp.float32).reshape(sequences, proposals, local_heads, head_size)

    key_scale = head_size ** (-0.5)
    cell_new, norm_new, new_max = fold_pending(
        state_cell,
        state_norm,
        state_max,
        split_heads(pend_keys) * key_scale,
        split_heads(pend_values),
        pend_gates,
        forget_bias,
        accepted,
    )
    log_in = gate_pre[:, :, 0, :]
    log_keep = jax.nn.log_sigmoid(gate_pre[:, :, 1, :] + forget_bias)
    hidden = read_block(
        split_heads(queries),
        split_heads(new_keys) * key_scale,
        split_heads(new_values),
        log_in,
        log_keep,
        cell_new,
        norm_new,
        new_max,
    )
    normed = hidden * lax.rsqrt(jnp.mean(hidden * hidden, axis=-1, keepdims=True) + epsilon)
    normed = normed * head_gain.reshape(local_heads, head_size)
    gated_rows = (jax.nn.sigmoid(split_heads(outgate)) * normed).astype(jnp.bfloat16)
    gated_rows = gated_rows.reshape(token_count, local_heads * head_size)
    mixed_out = mix_by_digits(gated_rows, far_mix, model_width)
    return (mixed_out.reshape(sequences, proposals, -1), cell_new, norm_new, new_max)


def solution(mesh):
    return jax.shard_map(
        shards,
        mesh=mesh,
        in_specs=(
            P("kv", None, None),
            P(),
            P("kv", "tp"),
            P("kv", "tp"),
            P("kv", "tp"),
            P("kv", "tp"),
            P("kv", None, "tp"),
            P("tp"),
            P("tp"),
            P("tp", "kv"),
            P("kv", "tp", None, None),
            P("kv", "tp", None),
            P("kv", "tp"),
            P("kv", None, "tp"),
            P("kv", None, "tp"),
            P("kv", None, None, "tp"),
            P("kv"),
        ),
        out_specs=(
            P("kv", None, "tp"),
            P("kv", "tp", None, None),
            P("kv", "tp", None),
            P("kv", "tp"),
        ),
        check_vma=False,
    )
```
